32 devices in a mesh: sp: 8 (over z, core), tp: 4 (over y, x).
Axes of the slice: x: 2, y: 2, z: 4, core: 2. Of those that a mesh axis runs over, the one named last changes fastest.
Arguments:
- layer_input: bfloat16 [8192, 4096], P('sp', 'tp'), may hold values from -6 to 6
- key_weight: bfloat16 [4096, 4096], P(None, 'tp'), may hold values from -0.09375 to 0.09375
- value_weight: bfloat16 [4096, 4096], P(None, 'tp'), may hold values from -0.09375 to 0.09375
- decay_exponent: float32 [32], P('tp'), may hold values from -0.077 to -0.00016845703, as said below
- query_new: bfloat16 [2, 4096], P(None, 'tp'), may hold values from -6 to 6
- key_new: bfloat16 [2, 4096], P(None, 'tp'), may hold values from -6 to 6
- value_new: bfloat16 [2, 4096], P(None, 'tp'), may hold values from -6 to 6
- norm_gain: float32 [4096], P('tp'), may hold values from 0.1 to 1.9
Outputs:
- state_cache: bfloat16 [2, 32, 128, 128], P(None, 'tp', 'sp')
- first_read: bfloat16 [2, 4096], P(None, 'tp')
The draws below stay inside these ranges and needn't reach their ends.
Inputs may be any that keep to these rules, and one draw needn't show every extreme that they name: decay_exponent is negative.
All inputs are finite; a program needn't handle non-finite values.
Results may differ from the reference program's by a relative error of at most 0.011.
Values may be sent and summed in bfloat16 or wider, within the bound.
A program may use at most 64 MiB of HBM per device.

```python
import jax
import jax.numpy as jnp
from jax import lax

D = 4096
HEADS = 32
DK = 128
DV = 128
SEQS = 2
TOKENS = 8192
LEN = 4096


def draw_decay_exponent(key, part):
    first_key = jax.random.fold_in(key, 11)
    second_key = jax.random.fold_in(key, 12)
    third_key = jax.random.fold_in(key, 13)
    slow_share = 0.5
    slow_flag = jax.random.uniform(first_key, (HEADS,), jnp.float32) < slow_share
    fast_rate = jax.random.uniform(second_key, (HEADS,), jnp.float32, 2.3026 / 100.0, 2.3026 / 30.0)
    slow_rate = jax.random.uniform(third_key, (HEADS,), jnp.float32, 0.3, 1.0) * (2.3026 / LEN)
    return -jnp.where(slow_flag, slow_rate, fast_rate)


def levels(rng, dims, shards, least, largest):
    def one(dim, parts):
        draws = jax.random.uniform(jax.random.fold_in(jax.random.fold_in(rng, 6), dim), (parts,), jnp.float32, least / len(shards), largest / len(shards))
        return jnp.repeat(jnp.exp(draws), dims[dim] // parts).reshape((-1,) + (1,) * (len(dims) - dim - 1))

    gain = one(*shards[0])
    for cut in shards[1:]:
        gain = gain * one(*cut)
    return gain


def bell_draw(stream_key, extent, spread, most, split=(), kind=jnp.bfloat16):
    result = spread * jax.random.normal(stream_key, extent, jnp.float32)
    if split:
        result = result * levels(stream_key, extent, split, -0.22, 0.18)
    return jnp.clip(result, -most, most).astype(kind)


def setup_inputs(seed: int = 0) -> dict:
    key_of = jax.random.split(jax.random.key(seed), 9)
    return {
        "layer_input": bell_draw(key_of[0], (TOKENS, D), 1.0, 6.0, ((0, 8), (1, 4))),
        "key_weight": bell_draw(key_of[1], (D, HEADS * DK), D ** -0.5, 0.09375, ((1, 4),)),
        "value_weight": bell_draw(key_of[2], (D, HEADS * DV), D ** -0.5, 0.09375, ((1, 4),)),
        "decay_exponent": draw_decay_exponent(jax.random.fold_in(key_of[8], 71), 0),
        "query_new": bell_draw(key_of[4], (SEQS, HEADS * DK), 1.0, 6.0, ((1, 4),)),
        "key_new": bell_draw(key_of[5], (SEQS, HEADS * DK), 1.0, 6.0, ((1, 4),)),
        "value_new": bell_draw(key_of[6], (SEQS, HEADS * DV), 1.0, 6.0, ((1, 4),)),
        "norm_gain": jnp.clip(1.0 + 0.18 * jax.random.normal(key_of[7], (HEADS * DV,), jnp.float32), 0.1, 1.9),
    }


def rotate(projected, position):
    half_width = projected.shape[-1] // 2
    inverse = 1.0 / 10000.0 ** jnp.linspace(0.0, 1.0, half_width, dtype=jnp.float32)
    angle = position[:, None] * inverse[None, :]
    cosine = jnp.cos(angle)[:, None, :]
    sine = jnp.sin(angle)[:, None, :]
    first = projected[..., :half_width]
    second = projected[..., half_width:]
    return jnp.concatenate([first * cosine - second * sine, first * sine + second * cosine], axis=-1)

def reference(layer_input, key_weight, value_weight, decay_exponent, query_new, key_new, value_new, norm_gain):
    key_proj = jnp.dot(layer_input, key_weight, preferred_element_type=jnp.float32)
    value_proj = jnp.dot(layer_input, value_weight, preferred_element_type=jnp.float32)
    position = (jnp.arange(TOKENS, dtype=jnp.int32) % LEN).astype(jnp.float32)
    keys = (rotate(key_proj.reshape(TOKENS, HEADS, DK), position) * DK ** (-0.5)).astype(jnp.bfloat16)
    values = value_proj.astype(jnp.bfloat16).reshape(TOKENS, HEADS, DV)
    distance = LEN - 1.0 - position
    weighting = jnp.exp(decay_exponent[None, :] * distance[:, None])
    weighted = (keys.astype(jnp.float32) * weighting[:, :, None]).astype(jnp.bfloat16)
    final = jnp.einsum('slhd,slhe->shde', weighted.astype(jnp.float32).reshape(SEQS, LEN, HEADS, DK), values.astype(jnp.float32).reshape(SEQS, LEN, HEADS, DV), precision=lax.Precision.HIGHEST)
    state_cache = final.astype(jnp.bfloat16)
    queries = query_new.astype(jnp.float32).reshape(SEQS, HEADS, DK)
    keys_next = key_new.astype(jnp.float32).reshape(SEQS, HEADS, DK)
    values_next = value_new.astype(jnp.float32).reshape(SEQS, HEADS, DV)
    carried = jnp.einsum('shd,shde->she', queries, final, precision=lax.Precision.HIGHEST)
    own_term = lax.optimization_barrier(jnp.sum(queries * keys_next, axis=2))[:, :, None] * values_next
    mixed = jnp.exp(decay_exponent)[None, :, None] * carried + own_term
    normed = mixed * lax.rsqrt(lax.optimization_barrier(jnp.mean(mixed * mixed, axis=2, keepdims=True)) + 1e-06)
    normed = normed * norm_gain.reshape(HEADS, DV)[None, :, :]
    return (state_cache, normed.reshape(SEQS, HEADS * DV).astype(jnp.bfloat16))
```

```python
import functools
import math

import jax
import jax.numpy as jnp
import numpy as np
from jax import lax
from jax.experimental import pallas as pl
from jax.experimental.pallas import tpu as pltpu
from jax.sharding import PartitionSpec as P

SEQS = 2
CHUNKS = 8
LEAD = 1
VMEM_KIB = 48 * 1024
MESH = pl.DeviceIdType.MESH
F32 = jnp.float32
BF16 = jnp.bfloat16


def gather_kernel(
    side, seq_span, chunks,
    decay_hbm, inv_hbm, query_hbm, key_hbm, value_hbm, gain_hbm, x_ref, wk_ref, wv_ref,
    cache_ref, first_ref,
    decay_ref, inv_ref, query_ref, key_ref, value_ref, gain_ref,
    gx, wk, wv, cosine, sine, acc_k, acc_v,
    state_ref, query_wide, own_term, factor, staged, landed, read, reads,
    send_sem, recv_sem, local_sem, state_send, state_recv, read_send, read_recv, go_sem,
):
    tokens, feats = x_ref.shape
    rows = tokens // chunks
    half = rows // 2
    heads, width, vwidth = state_ref.shape
    pair = next(p for p in (4, 2, 1) if heads % p == 0)
    me = lax.axis_index("tp")
    my_y, my_x = me // side, lax.rem(me, side)
    sp_place = lax.axis_index("sp")
    sp_size = landed.shape[0]
    kept = landed.shape[2]
    groups = heads // pair
    core = lax.rem(sp_place, 2)

    def mirror(m):
        place, bit = 0, 1
        while bit < sp_size:
            flag = lax.rem(sp_place // bit + (m // bit) % 2, 2)
            place, bit = place + flag * bit, bit * 2
        return place

    sp_peers = [mirror(m) for m in range(sp_size - 1, 0, -1)]

    def x_peer(d):
        return my_y * side + lax.rem(my_x + d, side)

    def y_peer(d):
        return lax.rem(my_y + d, side) * side + my_x

    x_peers = [x_peer(d) for d in range(1, side)]
    y_peers = [y_peer(d) for d in range(1, side)]

    fetch = pltpu.make_async_copy(x_ref, gx.at[me], local_sem.at[0])
    fetch.start()
    barrier = pltpu.get_barrier_semaphore()
    for peer in x_peers + y_peers:
        pl.semaphore_signal(barrier, inc=1, device_id={"tp": peer}, device_id_type=MESH)
    for peer in sp_peers:
        pl.semaphore_signal(barrier, inc=1, device_id={"sp": peer}, device_id_type=MESH)
    pl.semaphore_wait(barrier, 2 * (side - 1) + sp_size - 1)

    def span(c, part):
        return pl.ds(pl.multiple_of(c * rows + part * half, half), half)

    def remote(c, slot, block, part, target):
        where = span(c, part)
        return pltpu.make_async_remote_copy(
            src_ref=gx.at[block, where],
            dst_ref=gx.at[block, where],
            send_sem=send_sem.at[c, slot],
            recv_sem=recv_sem.at[c, block, part],
            device_id={"tp": target},
            device_id_type=MESH,
        )

    fan = 2 * (side - 1)

    def own_copies(c, wave):
        out, slot = [], wave * fan
        for peers, part in ((x_peers, wave), (y_peers, 1 - wave)):
            for peer in peers:
                out.append(remote(c, slot, me, part, peer))
                slot += 1
        return out

    def relay_copies(c):
        out, slot = [], 2 * fan
        for part, sources, peers in ((0, x_peers, y_peers), (1, y_peers, x_peers)):
            for source in sources:
                for peer in peers:
                    out.append(remote(c, slot, source, part, peer))
                    slot += 1
        return out

    def arrived(c, block, part):
        remote(c, 0, block, part, x_peers[0]).wait_recv()

    late_blocks = [
        lax.rem(my_y + dy, side) * side + lax.rem(my_x + dx, side)
        for dy in range(1, side)
        for dx in range(1, side)
    ]

    def wait_wave(c, wave):
        for block in x_peers:
            arrived(c, block, wave)
        for block in y_peers:
            arrived(c, block, 1 - wave)

    def wait_late(c):
        for block in late_blocks:
            for part in range(2):
                arrived(c, block, part)

    def start_all(copies):
        for copy in copies:
            copy.start()

    def drain(copies):
        for copy in copies:
            copy.wait_send()

    fetch.wait()

    @pl.when(core == 1)
    def _():
        pl.semaphore_wait(go_sem, 1)

    def send_wave(wave):
        def body(c, _):
            start_all(own_copies(c, wave))
            return 0

        lax.fori_loop(0, chunks, body, 0)

    send_wave(0)
    send_wave(1)

    small = [
        pltpu.make_async_copy(source, target, local_sem.at[3 + i])
        for i, (source, target) in enumerate((
            (decay_hbm, decay_ref), (inv_hbm, inv_ref), (query_hbm, query_ref),
            (key_hbm, key_ref), (value_hbm, value_ref), (gain_hbm, gain_ref),
        ))
    ]
    for copy in small:
        copy.start()
    local = [
        pltpu.make_async_copy(wk_ref, wk, local_sem.at[1]),
        pltpu.make_async_copy(wv_ref, wv, local_sem.at[2]),
    ]
    for copy in local:
        copy.start()
    state_ref[...] = jnp.zeros_like(state_ref)

    def pass_on(c):
        wait_wave(c, 0)
        start_all(relay_copies(c))

    def pass_on_loop(c, _):
        pass_on(c)
        return 0

    lead = min(LEAD, chunks)
    lax.fori_loop(0, lead, pass_on_loop, 0)

    @pl.when(core == 0)
    def _():
        pl.semaphore_signal(go_sem, inc=1, device_id={"sp": sp_place + 1}, device_id_type=MESH)

    for copy in small:
        copy.wait()
    base = lax.rem(sp_place, seq_span) * tokens

    def table(c, _):
        at = pl.ds(pl.multiple_of(c * half, half), half)
        place = (base + c * half + lax.broadcasted_iota(jnp.int32, (half, width), 0)).astype(F32)
        angle = place * inv_ref[...]
        low = lax.broadcasted_iota(jnp.int32, (half, width), 1) < width // 2
        sin = jnp.sin(angle)
        cosine[at, :] = jnp.cos(angle)
        sine[at, :] = jnp.where(low, -sin, sin)
        return 0

    lax.fori_loop(0, 2 * chunks, table, 0)

    prompt = sp_place // seq_span
    diagonal = lax.broadcasted_iota(jnp.int32, (width, width), 0) == lax.broadcasted_iota(
        jnp.int32, (width, width), 1
    )
    ones = jnp.ones((width, vwidth), BF16)
    queries = query_ref[...].astype(F32)
    next_keys = key_ref[...].astype(F32)
    next_values = value_ref[...].astype(F32)
    for h in range(heads):
        cols = slice(h * width, (h + 1) * width)
        vcols = slice(h * vwidth, (h + 1) * vwidth)
        mine = jnp.zeros((1, width), F32)
        for s in range(SEQS):
            mine = jnp.where(prompt == s, queries[s:s + 1, cols], mine)
            score = jnp.sum(
                queries[s:s + 1, cols] * next_keys[s:s + 1, cols], axis=1, keepdims=True
            )
            own_term[s, h] = score * next_values[s:s + 1, vcols]
        spread = jnp.where(diagonal, jnp.broadcast_to(mine, (width, width)), 0.0).astype(BF16)
        query_wide[h] = jnp.dot(spread, ones, preferred_element_type=F32)
        factor[h] = jnp.exp(jnp.full((1, vwidth), decay_ref[h], F32))

    def state_copies(g):
        piece = pl.ds(g * pair, pair)
        return [
            pltpu.make_async_remote_copy(
                src_ref=staged.at[peer, piece],
                dst_ref=landed.at[sp_place, piece],
                send_sem=state_send.at[g, d],
                recv_sem=state_recv.at[g, sp_place],
                device_id={"sp": peer},
                device_id_type=MESH,
            )
            for d, peer in enumerate(sp_peers)
        ]

    def read_copies():
        return [
            pltpu.make_async_remote_copy(
                src_ref=read,
                dst_ref=reads.at[sp_place],
                send_sem=read_send.at[d],
                recv_sem=read_recv.at[sp_place],
                device_id={"sp": peer},
                device_id_type=MESH,
            )
            for d, peer in enumerate(sp_peers)
        ]

    for copy in local:
        copy.wait()

    def partial(c, blocks, w, cols):
        at = pl.ds(pl.multiple_of(c * rows, rows), rows)
        total = None
        for block in blocks:
            depth = pl.ds(pl.multiple_of(block * feats, feats), feats)
            term = jnp.dot(gx[block, at, :], w[depth, cols], preferred_element_type=F32)
            total = term if total is None else total + term
        return total

    early_blocks = [me] + x_peers + y_peers

    def early(c, _):
        wait_wave(c, 1)
        at = pl.ds(pl.multiple_of(c * rows, rows), rows)

        def step(g, _):
            kcols = pl.ds(pl.multiple_of(g * pair * width, pair * width), pair * width)
            vcols = pl.ds(pl.multiple_of(g * pair * vwidth, pair * vwidth), pair * vwidth)
            acc_k[at, kcols] = partial(c, early_blocks, wk, kcols)
            acc_v[at, vcols] = partial(c, early_blocks, wv, vcols)
            return 0

        lax.fori_loop(0, groups, step, 0)
        return 0

    def finish(c, last):
        wait_late(c)
        at = pl.ds(pl.multiple_of(c * rows, rows), rows)
        distance = (seq_span * tokens - 1 - base - c * rows) - lax.broadcasted_iota(
            jnp.int32, (rows, width), 0
        )
        distance = distance.astype(F32)

        def step(g, _):
            kcols = pl.ds(pl.multiple_of(g * pair * width, pair * width), pair * width)
            vcols = pl.ds(pl.multiple_of(g * pair * vwidth, pair * vwidth), pair * vwidth)
            k = partial(c, late_blocks, wk, kcols) + acc_k[at, kcols]
            v = partial(c, late_blocks, wv, vcols) + acc_v[at, vcols]
            v = v.astype(BF16)
            for j in range(pair):
                kh = k[:, j * width:(j + 1) * width]
                turned = kh * cosine[at, :] + pltpu.roll(kh, width // 2, 1) * sine[at, :]
                keys = (turned * width ** (-0.5)).astype(BF16).astype(F32)
                weighted = (keys * jnp.exp(decay_ref[g * pair + j] * distance)).astype(BF16)
                state_ref[g * pair + j] += lax.dot_general(
                    weighted, v[:, j * vwidth:(j + 1) * vwidth],
                    (((0,), (0,)), ((), ())), preferred_element_type=F32,
                )
            if last:
                for j in range(pair):
                    h = g * pair + j
                    held = state_ref[h]
                    for d in range(sp_size):
                        staged[d, h] = held[d * kept:(d + 1) * kept, :].astype(BF16)
                    read[h] = jnp.sum(query_wide[h] * held, axis=0, keepdims=True)
                start_all(state_copies(g))
            return 0

        lax.fori_loop(0, groups, step, 0)

    def finish_loop(c, _):
        finish(c, False)
        return 0

    def drain_wave(wave):
        def body(c, _):
            drain(own_copies(c, wave))
            return 0

        lax.fori_loop(0, chunks, body, 0)

    def drain_relay(c, _):
        drain(relay_copies(c))
        return 0

    lax.fori_loop(lead, chunks, pass_on_loop, 0)
    lax.fori_loop(0, chunks, early, 0)
    lax.fori_loop(0, chunks - 1, finish_loop, 0)
    drain_wave(0)
    drain_wave(1)
    finish(chunks - 1, True)

    start_all(read_copies())
    landed[sp_place] = staged[sp_place]
    reads[sp_place] = read[...]
    lax.fori_loop(0, chunks, drain_relay, 0)

    for d, peer in enumerate(sp_peers):
        pltpu.make_async_remote_copy(
            src_ref=read, dst_ref=reads.at[peer], send_sem=read_send.at[d],
            recv_sem=read_recv.at[peer], device_id={"sp": peer}, device_id_type=MESH,
        ).wait_recv()
        for g in range(groups):
            piece = pl.ds(g * pair, pair)
            pltpu.make_async_remote_copy(
                src_ref=staged.at[peer, piece], dst_ref=landed.at[peer, piece],
                send_sem=state_send.at[g, d], recv_sem=state_recv.at[g, peer],
                device_id={"sp": peer}, device_id_type=MESH,
            ).wait_recv()

    row = lax.broadcasted_iota(jnp.int32, (SEQS, heads * vwidth), 0)
    out = jnp.zeros((SEQS, heads * vwidth), F32)
    for s in range(SEQS):
        members = range(s * seq_span, (s + 1) * seq_span)
        carried = functools.reduce(jnp.add, [reads[m] for m in members])
        mixed = factor[...] * carried + own_term[s]
        normed = mixed * lax.rsqrt(jnp.mean(mixed * mixed, axis=2, keepdims=True) + 1e-06)
        line = jnp.concatenate([normed[h] for h in range(heads)], axis=1) * gain_ref[...]
        out = jnp.where(row == s, jnp.broadcast_to(line, out.shape), out)
        for h in range(heads):
            cache_ref[s, h] = functools.reduce(
                jnp.add, [landed[m, h].astype(F32) for m in members]
            ).astype(BF16)
    first_ref[...] = out.astype(BF16)

    for copy in read_copies():
        copy.wait_send()
    for g in range(groups):
        for copy in state_copies(g):
            copy.wait_send()


def settle(cache_ref, first_ref, cache_out, first_out):
    cache_out[...] = cache_ref[...]
    first_out[...] = first_ref[...]


def on_device(
    layer_input, key_weight, value_weight, decay_exponent, query_new, key_new, value_new, norm_gain
):
    tokens, feats = layer_input.shape
    parts = lax.axis_size("tp")
    sp_size = lax.axis_size("sp")
    seq_span = sp_size // SEQS
    side = math.isqrt(parts)
    heads = decay_exponent.shape[0]
    width = key_weight.shape[1] // heads
    vwidth = value_weight.shape[1] // heads
    kept = width // sp_size
    groups = heads // next(p for p in (4, 2, 1) if heads % p == 0)
    steps = np.linspace(0.0, 1.0, width // 2, dtype=np.float32)
    inverse = (np.float32(1.0) / np.power(np.float32(10000.0), steps)).astype(np.float32)
    inverse = jnp.asarray(np.concatenate([inverse, inverse])[None, :])
    sends = 4 * (side - 1) + 2 * (side - 1) ** 2
    anywhere = pl.BlockSpec(memory_space=pltpu.HBM)
    vmem = pl.BlockSpec(memory_space=pltpu.VMEM)
    held = [
        pltpu.with_memory_space_constraint(part, pltpu.HBM)
        for part in (
            decay_exponent, inverse, query_new, key_new, value_new, norm_gain.reshape(1, -1),
            layer_input, key_weight, value_weight,
        )
    ]
    state_cache, first_read = pl.pallas_call(
        functools.partial(gather_kernel, side, seq_span, CHUNKS),
        out_shape=(
            jax.ShapeDtypeStruct((SEQS, heads, kept, vwidth), BF16),
            jax.ShapeDtypeStruct((SEQS, heads * vwidth), BF16),
        ),
        in_specs=[anywhere] * 9,
        out_specs=(vmem, vmem),
        scratch_shapes=[
            pltpu.SMEM((heads,), F32),
            pltpu.VMEM(inverse.shape, F32),
            pltpu.VMEM(query_new.shape, BF16),
            pltpu.VMEM(key_new.shape, BF16),
            pltpu.VMEM(value_new.shape, BF16),
            pltpu.VMEM((1, heads * vwidth), F32),
            pltpu.VMEM((parts, tokens, feats), BF16),
            pltpu.VMEM(key_weight.shape, BF16),
            pltpu.VMEM(value_weight.shape, BF16),
            pltpu.VMEM((tokens, width), F32),
            pltpu.VMEM((tokens, width), F32),
            pltpu.VMEM((tokens, heads * width), F32),
            pltpu.VMEM((tokens, heads * vwidth), F32),
            pltpu.VMEM((heads, width, vwidth), F32),
            pltpu.VMEM((heads, width, vwidth), F32),
            pltpu.VMEM((SEQS, heads, 1, vwidth), F32),
            pltpu.VMEM((heads, 1, vwidth), F32),
            pltpu.VMEM((sp_size, heads, kept, vwidth), BF16),
            pltpu.VMEM((sp_size, heads, kept, vwidth), BF16),
            pltpu.VMEM((heads, 1, vwidth), F32),
            pltpu.VMEM((sp_size, heads, 1, vwidth), F32),
            pltpu.SemaphoreType.DMA((CHUNKS, sends)),
            pltpu.SemaphoreType.DMA((CHUNKS, parts, 2)),
            pltpu.SemaphoreType.DMA((9,)),
            pltpu.SemaphoreType.DMA((groups, sp_size - 1)),
            pltpu.SemaphoreType.DMA((groups, sp_size)),
            pltpu.SemaphoreType.DMA((sp_size - 1,)),
            pltpu.SemaphoreType.DMA((sp_size,)),
            pltpu.SemaphoreType.REGULAR,
        ],
        compiler_params=pltpu.CompilerParams(
            collective_id=0, has_side_effects=True, vmem_limit_bytes=VMEM_KIB * 1024
        ),
    )(*held)
    return pl.pallas_call(
        settle,
        out_shape=(
            jax.ShapeDtypeStruct(state_cache.shape, BF16),
            jax.ShapeDtypeStruct(first_read.shape, BF16),
        ),
        in_specs=[vmem, vmem],
        out_specs=(vmem, vmem),
        compiler_params=pltpu.CompilerParams(vmem_limit_bytes=4 * 1024 * 1024),
    )(state_cache, first_read)


def solution(mesh):
    in_specs = (
        P("sp", "tp"),
        P(None, "tp"),
        P(None, "tp"),
        P("tp"),
        P(None, "tp"),
        P(None, "tp"),
        P(None, "tp"),
        P("tp"),
    )
    out_specs = (P(None, "tp", "sp", None), P(None, "tp"))
    return jax.shard_map(
        on_device, mesh=mesh, in_specs=in_specs, out_specs=out_specs, check_vma=False
    )
```

```python
import functools
import math

import jax
import jax.numpy as jnp
import numpy as np
from jax import lax
from jax.experimental import pallas as pl
from jax.experimental.pallas import tpu as pltpu
from jax.sharding import PartitionSpec as P

SEQS = 2
CHUNKS = 8
LEAD = 1
VMEM_KIB = 48 * 1024
MESH = pl.DeviceIdType.MESH
F32 = jnp.float32
BF16 = jnp.bfloat16


def gather_kernel(
    side, seq_span, chunks,
    decay_hbm, inv_hbm, query_hbm, key_hbm, value_hbm, gain_hbm, x_ref, wk_ref, wv_ref,
    cache_ref, first_ref,
    decay_ref, inv_ref, fresh_ref, gain_ref,
    gx, w_ref, cosine, sine, acc_k, acc_v,
    state_ref, query_wide, own_term, factor, staged, landed, read, reads,
    send_sem, recv_sem, local_sem, out_sem, go_sem, ready_sem,
):
    tokens, feats = x_ref.shape
    rows = tokens // chunks
    half = rows // 2
    heads, width, vwidth = state_ref.shape
    pair = next(p for p in (4, 2, 1) if heads % p == 0)
    me = lax.axis_index("tp")
    my_y, my_x = me // side, lax.rem(me, side)
    sp_place = lax.axis_index("sp")
    sp_size = landed.shape[0]
    kept = landed.shape[2]
    groups = heads // pair
    core = lax.rem(sp_place, 2)

    def mirror(m):
        place, bit = 0, 1
        while bit < sp_size:
            flag = lax.rem(sp_place // bit + (m // bit) % 2, 2)
            place, bit = place + flag * bit, bit * 2
        return place

    sp_peers = [mirror(m) for m in range(sp_size - 1, 0, -1)]

    def x_peer(d):
        return my_y * side + lax.rem(my_x + d, side)

    def y_peer(d):
        return lax.rem(my_y + d, side) * side + my_x

    x_peers = [x_peer(d) for d in range(1, side)]
    y_peers = [y_peer(d) for d in range(1, side)]

    def fetch(first):
        at = pl.ds(0, rows) if first else pl.ds(rows, tokens - rows)
        return pltpu.make_async_copy(x_ref.at[at], gx.at[me, at], local_sem.at[0 if first else 1])

    fetch(True).start()
    mate = sp_place + 1 - 2 * core
    barrier = pltpu.get_barrier_semaphore()
    for peer in x_peers + y_peers:
        pl.semaphore_signal(barrier, inc=1, device_id={"tp": peer}, device_id_type=MESH)
    pl.semaphore_signal(barrier, inc=1, device_id={"sp": mate}, device_id_type=MESH)

    def greet(peer, _):
        pl.semaphore_signal(barrier, inc=1, device_id={"sp": peer}, device_id_type=MESH)
        return 0

    above = sp_place - core + 2
    lax.fori_loop(above, sp_size, greet, 0)

    if chunks > 1:
        fetch(False).start()
    pl.semaphore_wait(barrier, 2 * (side - 1) + 1 + sp_place - core)

    def answer(peer, _):
        pl.semaphore_signal(ready_sem, inc=1, device_id={"sp": peer}, device_id_type=MESH)
        return 0

    def span(c, part):
        return pl.ds(pl.multiple_of(c * rows + part * half, half), half)

    def remote(c, slot, block, part, target, kind):
        where = span(c, part)
        return pltpu.make_async_remote_copy(
            src_ref=gx.at[block, where],
            dst_ref=gx.at[block, where],
            send_sem=send_sem.at[slot],
            recv_sem=recv_sem.at[kind, c],
            device_id={"tp": target},
            device_id_type=MESH,
        )

    fan = 2 * (side - 1)

    def own_copies(c, wave):
        out, slot = [], 0
        for peers, part in ((x_peers, wave), (y_peers, 1 - wave)):
            for peer in peers:
                out.append(remote(c, slot, me, part, peer, wave))
                slot += 1
        return out

    def relay_copies(c):
        out, slot = [], fan
        for part, sources, peers in ((0, x_peers, y_peers), (1, y_peers, x_peers)):
            for peer in peers:
                for source in sources:
                    out.append(remote(c, slot, source, part, peer, 2))
                slot += 1
        return out

    def arrived(c, kind, count):
        spot = gx.at[pl.ds(0, count), pl.ds(0, rows)]
        pltpu.make_async_copy(spot, spot, recv_sem.at[kind, c]).wait()

    late_blocks = [
        lax.rem(my_y + dy, side) * side + lax.rem(my_x + dx, side)
        for dy in range(1, side)
        for dx in range(1, side)
    ]

    def wait_wave(c, wave):
        arrived(c, wave, side - 1)

    def wait_late(c):
        arrived(c, 2, (side - 1) ** 2)

    def start_all(copies):
        for copy in copies:
            copy.start()

    def drain_own():
        for slot in range(fan):
            pltpu.make_async_copy(gx.at[0], gx.at[0], send_sem.at[slot]).wait()

    def drain_relay():
        half_block = pl.ds(0, tokens // 2)
        for slot in range(fan):
            blocks = gx.at[pl.ds(0, side - 1), half_block]
            pltpu.make_async_copy(blocks, blocks, send_sem.at[fan + slot]).wait()

    @pl.when(core == 1)
    def _():
        pl.semaphore_wait(go_sem, 1)

    def send_wave(wave):
        def body(c, _):
            start_all(own_copies(c, wave))
            return 0

        lax.fori_loop(1 if wave == 0 else 0, chunks, body, 0)

    fetch(True).wait()
    start_all(own_copies(0, 0))
    if chunks > 1:
        fetch(False).wait()
    send_wave(0)
    send_wave(1)
    lax.fori_loop(0, sp_place - core, answer, 0)

    small = [
        pltpu.make_async_copy(source, target, local_sem.at[2 + i])
        for i, (source, target) in enumerate((
            (decay_hbm, decay_ref), (inv_hbm, inv_ref), (gain_hbm, gain_ref),
        ))
    ]
    fresh = [
        pltpu.make_async_copy(source, fresh_ref.at[i], local_sem.at[5])
        for i, source in enumerate((query_hbm, key_hbm, value_hbm))
    ]
    weights = [
        pltpu.make_async_copy(source, w_ref.at[i], local_sem.at[6])
        for i, source in enumerate((wk_ref, wv_ref))
    ]
    start_all(small)
    start_all(fresh)
    start_all(weights)
    state_ref[...] = jnp.zeros_like(state_ref)

    def pass_on(c):
        wait_wave(c, 0)
        start_all(relay_copies(c))

    def pass_on_loop(c, _):
        pass_on(c)
        return 0

    lead = min(LEAD, chunks)
    lax.fori_loop(0, lead, pass_on_loop, 0)

    @pl.when(core == 0)
    def _():
        pl.semaphore_signal(go_sem, inc=1, device_id={"sp": sp_place + 1}, device_id_type=MESH)

    for copy in small:
        copy.wait()
    pltpu.make_async_copy(fresh_ref, fresh_ref, local_sem.at[5]).wait()
    base = lax.rem(sp_place, seq_span) * tokens

    def table(c, _):
        at = pl.ds(pl.multiple_of(c * half, half), half)
        place = (base + c * half + lax.broadcasted_iota(jnp.int32, (half, width), 0)).astype(F32)
        angle = place * inv_ref[...]
        low = lax.broadcasted_iota(jnp.int32, (half, width), 1) < width // 2
        sin = jnp.sin(angle)
        cosine[at, :] = jnp.cos(angle)
        sine[at, :] = jnp.where(low, -sin, sin)
        return 0

    lax.fori_loop(0, 2 * chunks, table, 0)

    prompt = sp_place // seq_span
    diagonal = lax.broadcasted_iota(jnp.int32, (width, width), 0) == lax.broadcasted_iota(
        jnp.int32, (width, width), 1
    )
    ones = jnp.ones((width, vwidth), BF16)
    queries, next_keys, next_values = (fresh_ref[i].astype(F32) for i in range(3))
    for h in range(heads):
        cols = slice(h * width, (h + 1) * width)
        vcols = slice(h * vwidth, (h + 1) * vwidth)
        mine = jnp.zeros((1, width), F32)
        for s in range(SEQS):
            mine = jnp.where(prompt == s, queries[s:s + 1, cols], mine)
            score = jnp.sum(
                queries[s:s + 1, cols] * next_keys[s:s + 1, cols], axis=1, keepdims=True
            )
            own_term[s, h] = score * next_values[s:s + 1, vcols]
        spread = jnp.where(diagonal, jnp.broadcast_to(mine, (width, width)), 0.0).astype(BF16)
        query_wide[h] = jnp.dot(spread, ones, preferred_element_type=F32)
        factor[h] = jnp.exp(jnp.full((1, vwidth), decay_ref[h], F32))

    def state_copies(g):
        piece = pl.ds(g * pair, pair)
        return [
            pltpu.make_async_remote_copy(
                src_ref=staged.at[peer, piece],
                dst_ref=landed.at[sp_place, piece],
                send_sem=out_sem.at[0],
                recv_sem=out_sem.at[1],
                device_id={"sp": peer},
                device_id_type=MESH,
            )
            for peer in sp_peers
        ]

    def read_copies(g):
        piece = pl.ds(g * pair, pair)
        return [
            pltpu.make_async_remote_copy(
                src_ref=read.at[piece],
                dst_ref=reads.at[sp_place, piece],
                send_sem=out_sem.at[2],
                recv_sem=out_sem.at[3],
                device_id={"sp": peer},
                device_id_type=MESH,
            )
            for peer in sp_peers
        ]

    def hand_out(g):
        for state_copy, read_copy in zip(state_copies(g), read_copies(g)):
            read_copy.start()
            state_copy.start()

    pltpu.make_async_copy(w_ref, w_ref, local_sem.at[6]).wait()
    wk, wv = w_ref.at[0], w_ref.at[1]

    def partial(c, blocks, w, cols):
        at = pl.ds(pl.multiple_of(c * rows, rows), rows)
        total = None
        for block in blocks:
            depth = pl.ds(pl.multiple_of(block * feats, feats), feats)
            term = jnp.dot(gx[block, at, :], w[depth, cols], preferred_element_type=F32)
            total = term if total is None else total + term
        return total

    early_blocks = [me] + x_peers + y_peers

    def early(c, _):
        wait_wave(c, 1)
        at = pl.ds(pl.multiple_of(c * rows, rows), rows)

        def step(g, _):
            kcols = pl.ds(pl.multiple_of(g * pair * width, pair * width), pair * width)
            vcols = pl.ds(pl.multiple_of(g * pair * vwidth, pair * vwidth), pair * vwidth)
            acc_k[at, kcols] = partial(c, early_blocks, wk, kcols)
            acc_v[at, vcols] = partial(c, early_blocks, wv, vcols)
            return 0

        lax.fori_loop(0, groups, step, 0)
        return 0

    def finish(c, last):
        wait_late(c)
        at = pl.ds(pl.multiple_of(c * rows, rows), rows)
        distance = (seq_span * tokens - 1 - base - c * rows) - lax.broadcasted_iota(
            jnp.int32, (rows, width), 0
        )
        distance = distance.astype(F32)

        def step(g, _):
            kcols = pl.ds(pl.multiple_of(g * pair * width, pair * width), pair * width)
            vcols = pl.ds(pl.multiple_of(g * pair * vwidth, pair * vwidth), pair * vwidth)
            k = partial(c, late_blocks, wk, kcols) + acc_k[at, kcols]
            v = partial(c, late_blocks, wv, vcols) + acc_v[at, vcols]
            v = v.astype(BF16)
            for j in range(pair):
                kh = k[:, j * width:(j + 1) * width]
                turned = kh * cosine[at, :] + pltpu.roll(kh, width // 2, 1) * sine[at, :]
                keys = (turned * width ** (-0.5)).astype(BF16).astype(F32)
                weighted = (keys * jnp.exp(decay_ref[g * pair + j] * distance)).astype(BF16)
                state_ref[g * pair + j] += lax.dot_general(
                    weighted, v[:, j * vwidth:(j + 1) * vwidth],
                    (((0,), (0,)), ((), ())), preferred_element_type=F32,
                )
            if last:
                for j in range(pair):
                    h = g * pair + j
                    held = state_ref[h]
                    for d in range(sp_size):
                        staged[d, h] = held[d * kept:(d + 1) * kept, :].astype(BF16)
                    read[h] = jnp.sum(query_wide[h] * held, axis=0, keepdims=True)
                hand_out(g)
            return 0

        lax.fori_loop(0, groups, step, 0)

    def finish_loop(c, _):
        finish(c, False)
        return 0

    lax.fori_loop(lead, chunks, pass_on_loop, 0)
    lax.fori_loop(0, chunks, early, 0)
    lax.fori_loop(0, chunks - 1, finish_loop, 0)
    drain_own()

    @pl.when(above < sp_size)
    def _():
        pl.semaphore_wait(ready_sem, sp_size - above)

    finish(chunks - 1, True)

    landed[sp_place] = staged[sp_place]
    reads[sp_place] = read[...]
    drain_relay()

    def exchanged(which):
        others = pl.ds(0, sp_size - 1)
        pltpu.make_async_copy(staged.at[others], landed.at[others], out_sem.at[which]).wait()
        pltpu.make_async_copy(reads.at[others], reads.at[others], out_sem.at[2 + which]).wait()

    exchanged(1)
    row = lax.broadcasted_iota(jnp.int32, (SEQS, heads * vwidth), 0)
    out = jnp.zeros((SEQS, heads * vwidth), F32)
    for s in range(SEQS):
        members = range(s * seq_span, (s + 1) * seq_span)
        carried = functools.reduce(jnp.add, [reads[m] for m in members])
        mixed = factor[...] * carried + own_term[s]
        normed = mixed * lax.rsqrt(jnp.mean(mixed * mixed, axis=2, keepdims=True) + 1e-06)
        line = jnp.concatenate([normed[h] for h in range(heads)], axis=1) * gain_ref[...]
        out = jnp.where(row == s, jnp.broadcast_to(line, out.shape), out)
        for h in range(heads):
            cache_ref[s, h] = functools.reduce(
                jnp.add, [landed[m, h].astype(F32) for m in members]
            ).astype(BF16)
    first_ref[...] = out.astype(BF16)

    exchanged(0)


def settle(cache_ref, first_ref, cache_out, first_out):
    cache_out[...] = cache_ref[...]
    first_out[...] = first_ref[...]


def on_device(
    layer_input, key_weight, value_weight, decay_exponent, query_new, key_new, value_new, norm_gain
):
    tokens, feats = layer_input.shape
    parts = lax.axis_size("tp")
    sp_size = lax.axis_size("sp")
    seq_span = sp_size // SEQS
    side = math.isqrt(parts)
    heads = decay_exponent.shape[0]
    width = key_weight.shape[1] // heads
    vwidth = value_weight.shape[1] // heads
    kept = width // sp_size
    steps = np.linspace(0.0, 1.0, width // 2, dtype=np.float32)
    inverse = (np.float32(1.0) / np.power(np.float32(10000.0), steps)).astype(np.float32)
    inverse = jnp.asarray(np.concatenate([inverse, inverse])[None, :])
    anywhere = pl.BlockSpec(memory_space=pltpu.HBM)
    vmem = pl.BlockSpec(memory_space=pltpu.VMEM)
    held = [
        pltpu.with_memory_space_constraint(part, pltpu.HBM)
        for part in (
            decay_exponent, inverse, query_new, key_new, value_new, norm_gain.reshape(1, -1),
            layer_input, key_weight, value_weight,
        )
    ]
    state_cache, first_read = pl.pallas_call(
        functools.partial(gather_kernel, side, seq_span, CHUNKS),
        out_shape=(
            jax.ShapeDtypeStruct((SEQS, heads, kept, vwidth), BF16),
            jax.ShapeDtypeStruct((SEQS, heads * vwidth), BF16),
        ),
        in_specs=[anywhere] * 9,
        out_specs=(vmem, vmem),
        scratch_shapes=[
            pltpu.SMEM((heads,), F32),
            pltpu.VMEM(inverse.shape, F32),
            pltpu.VMEM((3,) + query_new.shape, BF16),
            pltpu.VMEM((1, heads * vwidth), F32),
            pltpu.VMEM((parts, tokens, feats), BF16),
            pltpu.VMEM((2,) + key_weight.shape, BF16),
            pltpu.VMEM((tokens, width), F32),
            pltpu.VMEM((tokens, width), F32),
            pltpu.VMEM((tokens, heads * width), F32),
            pltpu.VMEM((tokens, heads * vwidth), F32),
            pltpu.VMEM((heads, width, vwidth), F32),
            pltpu.VMEM((heads, width, vwidth), F32),
            pltpu.VMEM((SEQS, heads, 1, vwidth), F32),
            pltpu.VMEM((heads, 1, vwidth), F32),
            pltpu.VMEM((sp_size, heads, kept, vwidth), BF16),
            pltpu.VMEM((sp_size, heads, kept, vwidth), BF16),
            pltpu.VMEM((heads, 1, vwidth), F32),
            pltpu.VMEM((sp_size, heads, 1, vwidth), F32),
            pltpu.SemaphoreType.DMA((4 * (side - 1),)),
            pltpu.SemaphoreType.DMA((3, CHUNKS)),
            pltpu.SemaphoreType.DMA((7,)),
            pltpu.SemaphoreType.DMA((4,)),
            pltpu.SemaphoreType.REGULAR,
            pltpu.SemaphoreType.REGULAR,
        ],
        compiler_params=pltpu.CompilerParams(
            collective_id=0, has_side_effects=True, vmem_limit_bytes=VMEM_KIB * 1024
        ),
    )(*held)
    return pl.pallas_call(
        settle,
        out_shape=(
            jax.ShapeDtypeStruct(state_cache.shape, BF16),
            jax.ShapeDtypeStruct(first_read.shape, BF16),
        ),
        in_specs=[vmem, vmem],
        out_specs=(vmem, vmem),
        compiler_params=pltpu.CompilerParams(vmem_limit_bytes=4 * 1024 * 1024),
    )(state_cache, first_read)


def solution(mesh):
    in_specs = (
        P("sp", "tp"),
        P(None, "tp"),
        P(None, "tp"),
        P("tp"),
        P(None, "tp"),
        P(None, "tp"),
        P(None, "tp"),
        P("tp"),
    )
    out_specs = (P(None, "tp", "sp", None), P(None, "tp"))
    return jax.shard_map(
        on_device, mesh=mesh, in_specs=in_specs, out_specs=out_specs, check_vma=False
    )
```

```python
import functools
import math

import jax
import jax.numpy as jnp
import numpy as np
from jax import lax
from jax.experimental import pallas as pl
from jax.experimental.pallas import tpu as pltpu
from jax.sharding import PartitionSpec as P

SEQS = 2
CHUNKS = 8
LEAD = 1
CUTS = 1
VMEM_KIB = 48 * 1024
MESH = pl.DeviceIdType.MESH
F32 = jnp.float32
BF16 = jnp.bfloat16


def gather_kernel(
    side, seq_span, chunks,
    decay_hbm, inv_hbm, query_hbm, key_hbm, value_hbm, gain_hbm, x_ref, wk_ref, wv_ref,
    cache_ref, first_ref,
    decay_ref, inv_ref, fresh_ref, gain_ref,
    gx, w_ref, cosine, sine, acc_k, acc_v,
    state_ref, fade, shrink, query_wide, own_term, factor, staged, landed, read, reads,
    send_sem, recv_sem, local_sem, out_sem, go_sem, ready_sem, x_sem, y_sem, mate_sem,
):
    tokens, feats = x_ref.shape
    rows = tokens // chunks
    half = rows // 2
    heads, width, vwidth = state_ref.shape
    pair = next(p for p in (4, 2, 1) if heads % p == 0)
    me = lax.axis_index("tp")
    my_y, my_x = me // side, lax.rem(me, side)
    sp_place = lax.axis_index("sp")
    sp_size = landed.shape[0]
    kept = landed.shape[2]
    groups = heads // pair
    core = lax.rem(sp_place, 2)

    def mirror(m):
        place, bit = 0, 1
        while bit < sp_size:
            flag = lax.rem(sp_place // bit + (m // bit) % 2, 2)
            place, bit = place + flag * bit, bit * 2
        return place

    sp_peers = [mirror(m) for m in range(sp_size - 1, 0, -1)]

    def x_peer(d):
        return my_y * side + lax.rem(my_x + d, side)

    def y_peer(d):
        return lax.rem(my_y + d, side) * side + my_x

    x_peers = [x_peer(d) for d in range(1, side)]
    y_peers = [y_peer(d) for d in range(1, side)]

    def fetch(first):
        at = pl.ds(0, rows) if first else pl.ds(rows, tokens - rows)
        return pltpu.make_async_copy(x_ref.at[at], gx.at[me, at], local_sem.at[0 if first else 1])

    fetch(True).start()
    barrier = pltpu.get_barrier_semaphore()
    below = sp_place - core
    above = below + 2

    def tell(semaphore, axis, peer):
        pl.semaphore_signal(semaphore, inc=1, device_id={axis: peer}, device_id_type=MESH)

    def expect(semaphore, count):
        @pl.when(count > 0)
        def _():
            pl.semaphore_wait(semaphore, count)

    for peer in x_peers + y_peers:
        pl.when(peer > me)(functools.partial(tell, barrier, "tp", peer))

    @pl.when(core == 0)
    def _():
        tell(barrier, "sp", sp_place + 1)

    def greet(peer, _):
        tell(barrier, "sp", peer)
        return 0

    lax.fori_loop(above, sp_size, greet, 0)
    expect(barrier, my_x + my_y + sp_place)
    for peer in x_peers:
        pl.when(peer < me)(functools.partial(tell, x_sem, "tp", peer))
    for peer in y_peers:
        pl.when(peer < me)(functools.partial(tell, y_sem, "tp", peer))

    @pl.when(core == 1)
    def _():
        tell(mate_sem, "sp", sp_place - 1)

    fetch(True).wait()
    if chunks > 1:
        fetch(False).start()

    def answer(peer, _):
        tell(ready_sem, "sp", peer)
        return 0

    def span(c, part):
        return pl.ds(pl.multiple_of(c * rows + part * half, half), half)

    def remote(c, slot, block, part, target, kind, cut=None):
        where = (block, span(c, part))
        if cut is not None:
            where += (pl.ds(cut * (feats // CUTS), feats // CUTS),)
        return pltpu.make_async_remote_copy(
            src_ref=gx.at[where],
            dst_ref=gx.at[where],
            send_sem=send_sem.at[slot],
            recv_sem=recv_sem.at[kind, c + (cut or 0)],
            device_id={"tp": target},
            device_id_type=MESH,
        )

    fan = 2 * (side - 1)

    def own_copies(c, wave, along_x):
        out, slot = [], 0 if along_x else side - 1
        for peer in x_peers if along_x else y_peers:
            part = wave if along_x else 1 - wave
            out.append(remote(c, slot, me, part, peer, wave))
            slot += 1
        return out

    def relay_copies(c, cuts=(None,)):
        out = []
        for cut in cuts:
            slot = fan
            for part, sources, peers in ((0, x_peers, y_peers), (1, y_peers, x_peers)):
                for peer in peers:
                    for source in sources:
                        out.append(remote(c, slot, source, part, peer, 2, cut))
                    slot += 1
        return out

    def arrived(c, kind, count, cuts=1):
        spot = gx.at[pl.ds(0, count), pl.ds(0, rows), pl.ds(0, feats // cuts)]
        pltpu.make_async_copy(spot, spot, recv_sem.at[kind, c]).wait()

    late_blocks = [
        lax.rem(my_y + dy, side) * side + lax.rem(my_x + dx, side)
        for dy in range(1, side)
        for dx in range(1, side)
    ]

    def wait_wave(c, wave):
        arrived(c, wave, side - 1)

    def wait_late(c, cuts=1):
        arrived(c, 2, (side - 1) ** 2, cuts)

    def start_all(copies):
        for copy in copies:
            copy.start()

    def drain_own():
        for slot in range(fan):
            pltpu.make_async_copy(gx.at[0], gx.at[0], send_sem.at[slot]).wait()

    def drain_relay():
        half_block = pl.ds(0, tokens // 2)
        for slot in range(fan):
            blocks = gx.at[pl.ds(0, side - 1), half_block]
            pltpu.make_async_copy(blocks, blocks, send_sem.at[fan + slot]).wait()


    @pl.when(core == 1)
    def _():
        pl.semaphore_wait(go_sem, 1)

    def send_first(along_x):
        start_all(own_copies(0, 0, along_x))

    x_last, y_last = my_x == side - 1, my_y == side - 1
    pl.when(x_last)(functools.partial(send_first, True))
    pl.when(y_last)(functools.partial(send_first, False))

    @pl.when(jnp.logical_not(x_last))
    def _():
        expect(x_sem, side - 1 - my_x)
        send_first(True)

    @pl.when(jnp.logical_not(y_last))
    def _():
        expect(y_sem, side - 1 - my_y)
        send_first(False)

    if chunks > 1:
        fetch(False).wait()

    def send_wave(wave):
        def body(c, _):
            start_all(own_copies(c, wave, True) + own_copies(c, wave, False))
            return 0

        lax.fori_loop(1 - wave, chunks, body, 0)

    send_wave(0)
    send_wave(1)
    lax.fori_loop(0, below, answer, 0)

    small = [
        pltpu.make_async_copy(source, target, local_sem.at[2 + i])
        for i, (source, target) in enumerate((
            (decay_hbm, decay_ref), (inv_hbm, inv_ref), (gain_hbm, gain_ref),
        ))
    ]
    fresh = [
        pltpu.make_async_copy(source, fresh_ref.at[i], local_sem.at[5])
        for i, source in enumerate((query_hbm, key_hbm, value_hbm))
    ]
    weights = [
        pltpu.make_async_copy(source, w_ref.at[i], local_sem.at[6])
        for i, source in enumerate((wk_ref, wv_ref))
    ]
    start_all(small)
    start_all(fresh)
    start_all(weights)
    state_ref[...] = jnp.zeros_like(state_ref)

    def pass_on(c, cuts=(None,)):
        wait_wave(c, 0)
        start_all(relay_copies(c, cuts))

    def pass_on_loop(c, _):
        pass_on(c)
        return 0

    lead, last = min(LEAD, chunks - 1), chunks - 1
    lax.fori_loop(0, lead, pass_on_loop, 0)

    @pl.when(core == 0)
    def _():
        pl.semaphore_wait(mate_sem, 1)
        tell(go_sem, "sp", sp_place + 1)

    for copy in small:
        copy.wait()
    pltpu.make_async_copy(fresh_ref, fresh_ref, local_sem.at[5]).wait()
    base = lax.rem(sp_place, seq_span) * tokens

    scale = width ** (-0.5)

    def table(c, _):
        at = pl.ds(pl.multiple_of(c * half, half), half)
        place = (base + c * half + lax.broadcasted_iota(jnp.int32, (half, width), 0)).astype(F32)
        angle = place * inv_ref[...]
        low = lax.broadcasted_iota(jnp.int32, (half, width), 1) < width // 2
        sin = jnp.sin(angle) * scale
        cosine[at, :] = jnp.cos(angle) * scale
        sine[at, :] = jnp.where(low, -sin, sin)
        return 0

    lax.fori_loop(0, 2 * chunks, table, 0)
    distance = (seq_span * tokens - tokens - base + rows - 1) - lax.broadcasted_iota(
        jnp.int32, (rows, width), 0
    )
    distance = distance.astype(F32)

    def fading(h, _):
        fade[h] = jnp.exp(decay_ref[h] * distance)
        shrink[h] = jnp.exp(jnp.full((1, vwidth), decay_ref[h] * rows, F32))
        return 0

    lax.fori_loop(0, heads, fading, 0)

    prompt = sp_place // seq_span
    diagonal = lax.broadcasted_iota(jnp.int32, (width, width), 0) == lax.broadcasted_iota(
        jnp.int32, (width, width), 1
    )
    ones = jnp.ones((width, vwidth), BF16)
    queries, next_keys, next_values = (fresh_ref[i].astype(F32) for i in range(3))
    for h in range(heads):
        cols = slice(h * width, (h + 1) * width)
        vcols = slice(h * vwidth, (h + 1) * vwidth)
        mine = jnp.zeros((1, width), F32)
        for s in range(SEQS):
            mine = jnp.where(prompt == s, queries[s:s + 1, cols], mine)
            score = jnp.sum(
                queries[s:s + 1, cols] * next_keys[s:s + 1, cols], axis=1, keepdims=True
            )
            own_term[s, h] = score * next_values[s:s + 1, vcols]
        spread = jnp.where(diagonal, jnp.broadcast_to(mine, (width, width)), 0.0).astype(BF16)
        query_wide[h] = jnp.dot(spread, ones, preferred_element_type=F32)
        factor[h] = jnp.exp(jnp.full((1, vwidth), decay_ref[h], F32))

    def state_copies(g):
        piece = pl.ds(g * pair, pair)
        return [
            pltpu.make_async_remote_copy(
                src_ref=staged.at[peer, piece],
                dst_ref=landed.at[sp_place, piece],
                send_sem=out_sem.at[0],
                recv_sem=out_sem.at[1],
                device_id={"sp": peer},
                device_id_type=MESH,
            )
            for peer in sp_peers
        ]

    def read_copies(g):
        piece = pl.ds(g * pair, pair)
        return [
            pltpu.make_async_remote_copy(
                src_ref=read.at[piece],
                dst_ref=reads.at[sp_place, piece],
                send_sem=out_sem.at[2],
                recv_sem=out_sem.at[3],
                device_id={"sp": peer},
                device_id_type=MESH,
            )
            for peer in sp_peers
        ]

    def hand_out(g):
        for state_copy, read_copy in zip(state_copies(g), read_copies(g)):
            read_copy.start()
            state_copy.start()

    pltpu.make_async_copy(w_ref, w_ref, local_sem.at[6]).wait()
    wk, wv = w_ref.at[0], w_ref.at[1]

    def partial(c, blocks, w, cols, cut=0, cuts=1):
        at = pl.ds(pl.multiple_of(c * rows, rows), rows)
        deep = feats // cuts
        total = None
        for block in blocks:
            depth = pl.ds(pl.multiple_of(block * feats + cut * deep, deep), deep)
            term = jnp.dot(
                gx[block, at, pl.ds(cut * deep, deep)], w[depth, cols],
                preferred_element_type=F32,
            )
            total = term if total is None else total + term
        return total

    early_blocks = [me] + x_peers + y_peers

    def early(c, _):
        wait_wave(c, 1)
        at = pl.ds(pl.multiple_of(c * rows, rows), rows)

        def step(g, _):
            kcols = pl.ds(pl.multiple_of(g * pair * width, pair * width), pair * width)
            vcols = pl.ds(pl.multiple_of(g * pair * vwidth, pair * vwidth), pair * vwidth)
            acc_k[at, kcols] = partial(c, early_blocks, wk, kcols)
            acc_v[at, vcols] = partial(c, early_blocks, wv, vcols)
            return 0

        lax.fori_loop(0, groups, step, 0)
        return 0

    def columns(g):
        return (
            pl.ds(pl.multiple_of(g * pair * width, pair * width), pair * width),
            pl.ds(pl.multiple_of(g * pair * vwidth, pair * vwidth), pair * vwidth),
        )

    def head_start(c, cut):
        wait_late(c + cut, CUTS)
        at = pl.ds(pl.multiple_of(c * rows, rows), rows)

        def step(g, _):
            kcols, vcols = columns(g)
            acc_k[at, kcols] += partial(c, late_blocks, wk, kcols, cut, CUTS)
            acc_v[at, vcols] += partial(c, late_blocks, wv, vcols, cut, CUTS)
            return 0

        lax.fori_loop(0, groups, step, 0)

    def finish(c, last):
        if last:
            for cut in range(CUTS - 1):
                head_start(c, cut)
            wait_late(c + CUTS - 1, CUTS)
        else:
            wait_late(c)
        at = pl.ds(pl.multiple_of(c * rows, rows), rows)
        cut = (CUTS - 1, CUTS) if last else (0, 1)

        def step(g, _):
            kcols, vcols = columns(g)
            k = partial(c, late_blocks, wk, kcols, *cut) + acc_k[at, kcols]
            v = partial(c, late_blocks, wv, vcols, *cut) + acc_v[at, vcols]
            v = v.astype(BF16)
            for j in range(pair):
                h = g * pair + j
                kh = k[:, j * width:(j + 1) * width]
                turned = kh * cosine[at, :] + pltpu.roll(kh, width // 2, 1) * sine[at, :]
                held = state_ref[h] * shrink[h] + lax.dot_general(
                    (turned * fade[h]).astype(BF16), v[:, j * vwidth:(j + 1) * vwidth],
                    (((0,), (0,)), ((), ())), preferred_element_type=F32,
                )
                if last:
                    for d in range(sp_size):
                        staged[d, h] = held[d * kept:(d + 1) * kept, :].astype(BF16)
                    read[h] = jnp.sum(query_wide[h] * held, axis=0, keepdims=True)
                else:
                    state_ref[h] = held
            if last:
                hand_out(g)
            return 0

        lax.fori_loop(0, groups, step, 0)

    def finish_loop(c, _):
        finish(c, False)
        return 0

    lax.fori_loop(lead, last, pass_on_loop, 0)
    pass_on(last, range(CUTS))
    lax.fori_loop(0, chunks, early, 0)
    lax.fori_loop(0, chunks - 1, finish_loop, 0)
    drain_own()

    expect(ready_sem, sp_size - above)

    finish(chunks - 1, True)

    landed[sp_place] = staged[sp_place]
    reads[sp_place] = read[...]
    drain_relay()

    def exchanged(which):
        others = pl.ds(0, sp_size - 1)
        pltpu.make_async_copy(staged.at[others], landed.at[others], out_sem.at[which]).wait()
        pltpu.make_async_copy(reads.at[others], reads.at[others], out_sem.at[2 + which]).wait()

    exchanged(1)
    row = lax.broadcasted_iota(jnp.int32, (SEQS, heads * vwidth), 0)
    out = jnp.zeros((SEQS, heads * vwidth), F32)
    for s in range(SEQS):
        members = range(s * seq_span, (s + 1) * seq_span)
        carried = functools.reduce(jnp.add, [reads[m] for m in members])
        mixed = factor[...] * carried + own_term[s]
        normed = mixed * lax.rsqrt(jnp.mean(mixed * mixed, axis=2, keepdims=True) + 1e-06)
        line = jnp.concatenate([normed[h] for h in range(heads)], axis=1) * gain_ref[...]
        out = jnp.where(row == s, jnp.broadcast_to(line, out.shape), out)
        for h in range(heads):
            cache_ref[s, h] = functools.reduce(
                jnp.add, [landed[m, h].astype(F32) for m in members]
            ).astype(BF16)
    first_ref[...] = out.astype(BF16)

    exchanged(0)


def settle(cache_ref, first_ref, cache_out, first_out):
    cache_out[...] = cache_ref[...]
    first_out[...] = first_ref[...]


def on_device(
    layer_input, key_weight, value_weight, decay_exponent, query_new, key_new, value_new, norm_gain
):
    tokens, feats = layer_input.shape
    parts = lax.axis_size("tp")
    sp_size = lax.axis_size("sp")
    seq_span = sp_size // SEQS
    side = math.isqrt(parts)
    heads = decay_exponent.shape[0]
    width = key_weight.shape[1] // heads
    vwidth = value_weight.shape[1] // heads
    kept = width // sp_size
    steps = np.linspace(0.0, 1.0, width // 2, dtype=np.float32)
    inverse = (np.float32(1.0) / np.power(np.float32(10000.0), steps)).astype(np.float32)
    inverse = jnp.asarray(np.concatenate([inverse, inverse])[None, :])
    anywhere = pl.BlockSpec(memory_space=pltpu.HBM)
    vmem = pl.BlockSpec(memory_space=pltpu.VMEM)
    held = [
        pltpu.with_memory_space_constraint(part, pltpu.HBM)
        for part in (
            decay_exponent, inverse, query_new, key_new, value_new, norm_gain.reshape(1, -1),
            layer_input, key_weight, value_weight,
        )
    ]
    state_cache, first_read = pl.pallas_call(
        functools.partial(gather_kernel, side, seq_span, CHUNKS),
        out_shape=(
            jax.ShapeDtypeStruct((SEQS, heads, kept, vwidth), BF16),
            jax.ShapeDtypeStruct((SEQS, heads * vwidth), BF16),
        ),
        in_specs=[anywhere] * 9,
        out_specs=(vmem, vmem),
        scratch_shapes=[
            pltpu.SMEM((heads,), F32),
            pltpu.VMEM(inverse.shape, F32),
            pltpu.VMEM((3,) + query_new.shape, BF16),
            pltpu.VMEM((1, heads * vwidth), F32),
            pltpu.VMEM((parts, tokens, feats), BF16),
            pltpu.VMEM((2,) + key_weight.shape, BF16),
            pltpu.VMEM((tokens, width), F32),
            pltpu.VMEM((tokens, width), F32),
            pltpu.VMEM((tokens, heads * width), F32),
            pltpu.VMEM((tokens, heads * vwidth), F32),
            pltpu.VMEM((heads, width, vwidth), F32),
            pltpu.VMEM((heads, tokens // CHUNKS, width), F32),
            pltpu.VMEM((heads, 1, vwidth), F32),
            pltpu.VMEM((heads, width, vwidth), F32),
            pltpu.VMEM((SEQS, heads, 1, vwidth), F32),
            pltpu.VMEM((heads, 1, vwidth), F32),
            pltpu.VMEM((sp_size, heads, kept, vwidth), BF16),
            pltpu.VMEM((sp_size, heads, kept, vwidth), BF16),
            pltpu.VMEM((heads, 1, vwidth), F32),
            pltpu.VMEM((sp_size, heads, 1, vwidth), F32),
            pltpu.SemaphoreType.DMA((4 * (side - 1),)),
            pltpu.SemaphoreType.DMA((3, CHUNKS + CUTS - 1)),
            pltpu.SemaphoreType.DMA((7,)),
            pltpu.SemaphoreType.DMA((4,)),
            pltpu.SemaphoreType.REGULAR,
            pltpu.SemaphoreType.REGULAR,
            pltpu.SemaphoreType.REGULAR,
            pltpu.SemaphoreType.REGULAR,
            pltpu.SemaphoreType.REGULAR,
        ],
        compiler_params=pltpu.CompilerParams(
            collective_id=0, has_side_effects=True, vmem_limit_bytes=VMEM_KIB * 1024
        ),
    )(*held)
    return pl.pallas_call(
        settle,
        out_shape=(
            jax.ShapeDtypeStruct(state_cache.shape, BF16),
            jax.ShapeDtypeStruct(first_read.shape, BF16),
        ),
        in_specs=[vmem, vmem],
        out_specs=(vmem, vmem),
        compiler_params=pltpu.CompilerParams(vmem_limit_bytes=4 * 1024 * 1024),
    )(state_cache, first_read)


def solution(mesh):
    in_specs = (
        P("sp", "tp"),
        P(None, "tp"),
        P(None, "tp"),
        P("tp"),
        P(None, "tp"),
        P(None, "tp"),
        P(None, "tp"),
        P("tp"),
    )
    out_specs = (P(None, "tp", "sp", None), P(None, "tp"))
    return jax.shard_map(
        on_device, mesh=mesh, in_specs=in_specs, out_specs=out_specs, check_vma=False
    )
```

```python
import functools
import math

import jax
import jax.numpy as jnp
import numpy as np
from jax import lax
from jax.experimental import pallas as pl
from jax.experimental.pallas import tpu as pltpu
from jax.sharding import PartitionSpec as P

SEQS = 2
CHUNKS = 8
LEAD = 1
SLIP = 16
VMEM_KIB = 48 * 1024
MESH = pl.DeviceIdType.MESH
F32 = jnp.float32
BF16 = jnp.bfloat16


def gather_kernel(
    side, seq_span, chunks,
    decay_hbm, inv_hbm, query_hbm, key_hbm, value_hbm, gain_hbm, x_ref, wk_ref, wv_ref,
    cache_ref, first_ref,
    decay_ref, inv_ref, fresh_ref, gain_ref,
    gx, w_ref, cosine, sine, acc_k, acc_v,
    state_ref, fade, shrink, query_wide, own_term, factor, staged, landed, read, reads,
    k_tmp, v_tmp, guest_fade, guest_wide, guest_staged, guest_landed, guest_read, guest_reads,
    send_sem, recv_sem, slip_send, slip_recv, local_sem, out_sem, guest_sem,
    go_sem, ready_sem, x_sem, y_sem, mate_sem,
):
    tokens, feats = x_ref.shape
    rows = tokens // chunks
    half = rows // 2
    slip = SLIP
    last = chunks - 1
    heads, width, vwidth = state_ref.shape
    pair = next(p for p in (4, 2, 1) if heads % p == 0)
    me = lax.axis_index("tp")
    my_y, my_x = me // side, lax.rem(me, side)
    sp_place = lax.axis_index("sp")
    sp_size = landed.shape[0]
    kept = landed.shape[2]
    groups = heads // pair
    core = lax.rem(sp_place, 2)
    shift = sp_size - 2
    donor, host = sp_place >= shift, sp_place < 2
    full = jnp.logical_not(donor)

    sp_peers = [jnp.where(sp_place > p, p, p + 1) for p in range(sp_size - 1)]

    def x_peer(d):
        return my_y * side + lax.rem(my_x + d, side)

    def y_peer(d):
        return lax.rem(my_y + d, side) * side + my_x

    x_peers = [x_peer(d) for d in range(1, side)]
    y_peers = [y_peer(d) for d in range(1, side)]
    late_blocks = [
        lax.rem(my_y + dy, side) * side + lax.rem(my_x + dx, side)
        for dy in range(1, side)
        for dx in range(1, side)
    ]
    early_blocks = [me] + x_peers + y_peers

    def fetch(first):
        at = pl.ds(0, rows) if first else pl.ds(rows, tokens - rows)
        return pltpu.make_async_copy(x_ref.at[at], gx.at[me, at], local_sem.at[0 if first else 1])

    fetch(True).start()
    barrier = pltpu.get_barrier_semaphore()
    below = sp_place - core
    above = below + 2

    def tell(semaphore, axis, peer):
        pl.semaphore_signal(semaphore, inc=1, device_id={axis: peer}, device_id_type=MESH)

    def expect(semaphore, count):
        @pl.when(count > 0)
        def _():
            pl.semaphore_wait(semaphore, count)

    for peer in x_peers + y_peers:
        pl.when(peer > me)(functools.partial(tell, barrier, "tp", peer))

    @pl.when(core == 0)
    def _():
        tell(barrier, "sp", sp_place + 1)

    def greet(peer, _):
        tell(barrier, "sp", peer)
        return 0

    lax.fori_loop(above, sp_size, greet, 0)
    expect(barrier, my_x + my_y + sp_place)
    for peer in x_peers:
        pl.when(peer < me)(functools.partial(tell, x_sem, "tp", peer))
    for peer in y_peers:
        pl.when(peer < me)(functools.partial(tell, y_sem, "tp", peer))

    @pl.when(core == 1)
    def _():
        tell(mate_sem, "sp", sp_place - 1)

    fetch(True).wait()
    fetch(False).start()

    def answer(peer, _):
        tell(ready_sem, "sp", peer)
        return 0

    def chunk_plot(c, count):
        return (
            lambda part: pl.multiple_of(c * rows + part * half, half),
            count, lambda slot: send_sem.at[slot], lambda kind: recv_sem.at[kind, c],
        )

    def slip_plot(which):
        return (
            lambda part: tokens + part * slip if which else last * rows + (part + 1) * half - slip,
            slip, lambda slot: slip_send.at[which], lambda kind: slip_recv.at[which, kind],
        )

    last_plot, tail_plot, guest_plot = chunk_plot(last, half - slip), slip_plot(0), slip_plot(1)

    def remote(plot, slot, block, part, target, kind):
        start, count, send, recv = plot
        where = (block, pl.ds(start(part), count))
        return pltpu.make_async_remote_copy(
            src_ref=gx.at[where],
            dst_ref=gx.at[where],
            send_sem=send(slot),
            recv_sem=recv(kind),
            device_id={"tp": target},
            device_id_type=MESH,
        )

    fan = 2 * (side - 1)

    def along(plot, wave, on_x):
        part = wave if on_x else 1 - wave
        first = 0 if on_x else side - 1
        return [
            remote(plot, first + slot, me, part, peer, wave)
            for slot, peer in enumerate(x_peers if on_x else y_peers)
        ]

    def own_copies(plot, wave):
        return along(plot, wave, True) + along(plot, wave, False)

    def relay_copies(plot):
        out, slot = [], fan
        for part, sources, peers in ((0, x_peers, y_peers), (1, y_peers, x_peers)):
            for peer in peers:
                for source in sources:
                    out.append(remote(plot, slot, source, part, peer, 2))
                slot += 1
        return out

    def arrived(plot, kind):
        blocks = (side - 1) ** 2 if kind == 2 else side - 1
        spot = gx.at[pl.ds(0, blocks), pl.ds(0, 2 * plot[1])]
        pltpu.make_async_copy(spot, spot, plot[3](kind)).wait()

    def start_all(copies):
        for copy in copies:
            copy.start()

    def settled(blocks, count, semaphore):
        spot = gx.at[pl.ds(0, blocks), pl.ds(0, count)]
        pltpu.make_async_copy(spot, spot, semaphore).wait()

    def lend():
        return [
            pltpu.make_async_remote_copy(
                src_ref=gx.at[me, pl.ds(tail_plot[0](part), slip)],
                dst_ref=gx.at[me, pl.ds(guest_plot[0](part), slip)],
                send_sem=guest_sem.at[0],
                recv_sem=guest_sem.at[1],
                device_id={"sp": sp_place - shift},
                device_id_type=MESH,
            )
            for part in range(2)
        ]

    @pl.when(core == 1)
    def _():
        pl.semaphore_wait(go_sem, 1)

    def send_first(on_x):
        start_all(along(chunk_plot(0, half), 0, on_x))

    x_last, y_last = my_x == side - 1, my_y == side - 1
    pl.when(x_last)(functools.partial(send_first, True))
    pl.when(y_last)(functools.partial(send_first, False))

    @pl.when(jnp.logical_not(x_last))
    def _():
        expect(x_sem, side - 1 - my_x)
        send_first(True)

    @pl.when(jnp.logical_not(y_last))
    def _():
        expect(y_sem, side - 1 - my_y)
        send_first(False)

    fetch(False).wait()

    @pl.when(donor)
    def _():
        start_all(lend())
        for block in x_peers + y_peers + late_blocks:
            for part in range(2):
                gx[block, pl.ds(tail_plot[0](part), slip), :] = jnp.zeros((slip, feats), BF16)

    def send_own(wave):
        def body(c, _):
            start_all(own_copies(chunk_plot(c, half), wave))
            return 0

        lax.fori_loop(1 - wave, last, body, 0)
        start_all(own_copies(last_plot, wave))

        @pl.when(full)
        def _():
            start_all(own_copies(tail_plot, wave))

    send_own(0)
    lax.fori_loop(0, below, answer, 0)

    small = [
        pltpu.make_async_copy(source, target, local_sem.at[2 + i])
        for i, (source, target) in enumerate((
            (decay_hbm, decay_ref), (inv_hbm, inv_ref), (gain_hbm, gain_ref),
        ))
    ]
    fresh = [
        pltpu.make_async_copy(source, fresh_ref.at[i], local_sem.at[5])
        for i, source in enumerate((query_hbm, key_hbm, value_hbm))
    ]
    weights = [
        pltpu.make_async_copy(source, w_ref.at[i], local_sem.at[6])
        for i, source in enumerate((wk_ref, wv_ref))
    ]
    start_all(small)
    start_all(fresh)
    start_all(weights)
    state_ref[...] = jnp.zeros_like(state_ref)

    def pass_on(plot):
        arrived(plot, 0)
        start_all(relay_copies(plot))

    def pass_on_loop(c, _):
        pass_on(chunk_plot(c, half))
        return 0

    lax.fori_loop(0, LEAD, pass_on_loop, 0)

    @pl.when(core == 0)
    def _():
        pl.semaphore_wait(mate_sem, 1)
        tell(go_sem, "sp", sp_place + 1)

    for copy in small:
        copy.wait()
    pltpu.make_async_copy(fresh_ref, fresh_ref, local_sem.at[5]).wait()
    base = lax.rem(sp_place, seq_span) * tokens
    guest_place = lax.rem(sp_place + shift, sp_size)
    guest_base = lax.rem(guest_place, seq_span) * tokens
    scale = width ** (-0.5)

    def fill(at, count, first):
        place = (first + lax.broadcasted_iota(jnp.int32, (count, width), 0)).astype(F32)
        angle = place * inv_ref[...]
        low = lax.broadcasted_iota(jnp.int32, (count, width), 1) < width // 2
        sin = jnp.sin(angle) * scale
        cosine[pl.ds(at, count), :] = jnp.cos(angle) * scale
        sine[pl.ds(at, count), :] = jnp.where(low, -sin, sin)

    def table(c, _):
        fill(pl.multiple_of(c * half, half), half, base + c * half)
        return 0

    lax.fori_loop(0, 2 * chunks, table, 0)

    def to_end(first, count):
        return ((seq_span * tokens - 1 - first) - lax.broadcasted_iota(
            jnp.int32, (count, width), 0
        )).astype(F32)

    distance = to_end(base + tokens - rows, rows)

    def fading(h, _):
        fade[h] = jnp.exp(decay_ref[h] * distance)
        shrink[h] = jnp.exp(jnp.full((1, vwidth), decay_ref[h] * rows, F32))
        return 0

    lax.fori_loop(0, heads, fading, 0)

    diagonal = lax.broadcasted_iota(jnp.int32, (width, width), 0) == lax.broadcasted_iota(
        jnp.int32, (width, width), 1
    )
    ones = jnp.ones((width, vwidth), BF16)
    queries, next_keys, next_values = (fresh_ref[i].astype(F32) for i in range(3))

    def widen(target, prompt):
        for h in range(heads):
            mine = jnp.zeros((1, width), F32)
            for s in range(SEQS):
                mine = jnp.where(
                    prompt == s, queries[s:s + 1, h * width:(h + 1) * width], mine
                )
            spread = jnp.where(
                diagonal, jnp.broadcast_to(mine, (width, width)), 0.0
            ).astype(BF16)
            target[h] = jnp.dot(spread, ones, preferred_element_type=F32)

    widen(query_wide, sp_place // seq_span)
    for h in range(heads):
        cols = slice(h * width, (h + 1) * width)
        for s in range(SEQS):
            score = jnp.sum(
                queries[s:s + 1, cols] * next_keys[s:s + 1, cols], axis=1, keepdims=True
            )
            own_term[s, h] = score * next_values[s:s + 1, h * vwidth:(h + 1) * vwidth]
        factor[h] = jnp.exp(jnp.full((1, vwidth), decay_ref[h], F32))

    @pl.when(donor)
    def _():
        for part in range(2):
            at = pl.ds(tail_plot[0](part), slip)
            cosine[at, :] = jnp.zeros((slip, width), F32)
            sine[at, :] = jnp.zeros((slip, width), F32)

    @pl.when(host)
    def _():
        settled(1, 2 * slip, guest_sem.at[1])
        for wave in range(2):
            start_all(own_copies(guest_plot, wave))

    send_own(1)

    @pl.when(host)
    def _():
        for part in range(2):
            first = guest_base + tail_plot[0](part)
            fill(guest_plot[0](part), slip, first)
            gap = to_end(first, slip)
            for h in range(heads):
                guest_fade[h, pl.ds(part * slip, slip), :] = jnp.exp(decay_ref[h] * gap)
        widen(guest_wide, guest_place // seq_span)

    def outgoing(g, state, state_to, gist, gist_to, semaphores, at):
        piece = pl.ds(g * pair, pair)
        out = []
        for peer in sp_peers:
            for k, (source, target) in enumerate((
                (gist.at[piece], gist_to.at[sp_place, piece]),
                (state.at[peer, piece], state_to.at[sp_place, piece]),
            )):
                out.append(pltpu.make_async_remote_copy(
                    src_ref=source,
                    dst_ref=target,
                    send_sem=semaphores.at[at + 2 * k],
                    recv_sem=semaphores.at[at + 2 * k + 1],
                    device_id={"sp": peer},
                    device_id_type=MESH,
                ))
        return out

    pltpu.make_async_copy(w_ref, w_ref, local_sem.at[6]).wait()
    wk, wv = w_ref.at[0], w_ref.at[1]

    def partial(at, blocks, w, cols):
        total = None
        for block in blocks:
            depth = pl.ds(pl.multiple_of(block * feats, feats), feats)
            term = jnp.dot(gx[block, at, :], w[depth, cols], preferred_element_type=F32)
            total = term if total is None else total + term
        return total

    def columns(g):
        return (
            pl.ds(pl.multiple_of(g * pair * width, pair * width), pair * width),
            pl.ds(pl.multiple_of(g * pair * vwidth, pair * vwidth), pair * vwidth),
        )

    def chunk_rows(c):
        return pl.ds(pl.multiple_of(c * rows, rows), rows)

    guest_rows = pl.ds(tokens, 2 * slip)

    def begin(at):
        def step(g, _):
            kcols, vcols = columns(g)
            acc_k[at, kcols] = partial(at, early_blocks, wk, kcols)
            acc_v[at, vcols] = partial(at, early_blocks, wv, vcols)
            return 0

        lax.fori_loop(0, groups, step, 0)

    def early(c, _):
        arrived(chunk_plot(c, half), 1)
        begin(chunk_rows(c))
        return 0

    def finish(at, count, weigh, keep, after):
        some = pl.ds(0, count)

        def multiply(g):
            kcols = pl.ds(g * pair * width, pair * width)
            vcols = pl.ds(g * pair * vwidth, pair * vwidth)
            k_tmp[g, some, :] = partial(at, late_blocks, wk, kcols) + acc_k[at, kcols]
            v_tmp[g, some, :] = (
                partial(at, late_blocks, wv, vcols) + acc_v[at, vcols]
            ).astype(BF16)

        def absorb(g):
            for j in range(pair):
                kh = k_tmp[g, some, j * width:(j + 1) * width]
                turned = kh * cosine[at, :] + pltpu.roll(kh, width // 2, 1) * sine[at, :]
                keep(g * pair + j, lax.dot_general(
                    (turned * weigh[g * pair + j]).astype(BF16),
                    v_tmp[g, some, j * vwidth:(j + 1) * vwidth],
                    (((0,), (0,)), ((), ())), preferred_element_type=F32,
                ))
            after(g)

        multiply(0)
        for g in range(1, groups):
            multiply(g)
            absorb(g - 1)
        absorb(groups - 1)

    def keep_on(h, update):
        state_ref[h] = state_ref[h] * shrink[h] + update

    def late(c, _):
        arrived(chunk_plot(c, half), 2)
        finish(chunk_rows(c), rows, fade, keep_on, lambda g: None)
        return 0

    def cut_up(h, held, wide, state, gist):
        for d in range(sp_size):
            state[d, h] = held[d * kept:(d + 1) * kept, :].astype(BF16)
        gist[h] = jnp.sum(wide[h] * held, axis=0, keepdims=True)

    middle = chunks // 2
    lax.fori_loop(LEAD, middle, pass_on_loop, 0)

    @pl.when(host)
    def _():
        arrived(guest_plot, 1)
        pass_on(guest_plot)

    lax.fori_loop(middle, last, pass_on_loop, 0)
    pass_on(last_plot)
    pl.when(full)(functools.partial(pass_on, tail_plot))
    pl.when(host)(functools.partial(begin, guest_rows))
    lax.fori_loop(0, last, early, 0)
    arrived(last_plot, 1)
    pl.when(full)(functools.partial(arrived, tail_plot, 1))
    begin(chunk_rows(last))

    lax.fori_loop(0, middle, late, 0)
    expect(ready_sem, sp_size - above)

    @pl.when(host)
    def _():
        arrived(guest_plot, 2)
        finish(
            guest_rows, 2 * slip, guest_fade,
            lambda h, held: cut_up(h, held, guest_wide, guest_staged, guest_read),
            lambda g: start_all(outgoing(
                g, guest_staged, guest_landed, guest_read, guest_reads, guest_sem, 2
            )),
        )
        guest_landed[sp_place] = guest_staged[sp_place]
        guest_reads[sp_place] = guest_read[...]

    lax.fori_loop(middle, last, late, 0)
    for slot in range(fan):
        settled(1, tokens - 2 * slip, send_sem.at[slot])
    arrived(last_plot, 2)
    pl.when(full)(functools.partial(arrived, tail_plot, 2))
    finish(
        chunk_rows(last), rows, fade,
        lambda h, update: cut_up(
            h, state_ref[h] * shrink[h] + update, query_wide, staged, read
        ),
        lambda g: start_all(outgoing(g, staged, landed, read, reads, out_sem, 0)),
    )

    landed[sp_place] = staged[sp_place]
    reads[sp_place] = read[...]
    for slot in range(fan):
        settled(side - 1, tokens // 2 - slip, send_sem.at[fan + slot])
    moved = (4 * (side - 1) + 2 * (side - 1) ** 2) * slip
    pl.when(full)(functools.partial(settled, 1, moved, slip_send.at[0]))
    pl.when(donor)(functools.partial(settled, 1, 2 * slip, guest_sem.at[0]))
    pl.when(host)(functools.partial(settled, 1, moved, slip_send.at[1]))

    def exchanged(gist, state, count, semaphores, at):
        some = pl.ds(0, count)
        for k, target in enumerate((gist, state)):
            pltpu.make_async_copy(
                target.at[some], target.at[some], semaphores.at[at + 2 * k]
            ).wait()

    pl.when(host)(functools.partial(exchanged, guest_reads, guest_landed, 1, guest_sem, 3))
    pl.when(jnp.logical_not(host))(
        functools.partial(exchanged, guest_reads, guest_landed, 2, guest_sem, 3)
    )
    exchanged(reads, landed, sp_size - 1, out_sem, 1)
    row = lax.broadcasted_iota(jnp.int32, (SEQS, heads * vwidth), 0)
    out = jnp.zeros((SEQS, heads * vwidth), F32)
    for s in range(SEQS):
        members = range(s * seq_span, (s + 1) * seq_span)
        guests = range(2) if s == SEQS - 1 else ()
        carried = functools.reduce(
            jnp.add, [reads[m] for m in members] + [guest_reads[m] for m in guests]
        )
        mixed = factor[...] * carried + own_term[s]
        normed = mixed * lax.rsqrt(jnp.mean(mixed * mixed, axis=2, keepdims=True) + 1e-06)
        line = jnp.concatenate([normed[h] for h in range(heads)], axis=1) * gain_ref[...]
        out = jnp.where(row == s, jnp.broadcast_to(line, out.shape), out)
        for h in range(heads):
            cache_ref[s, h] = functools.reduce(
                jnp.add,
                [landed[m, h].astype(F32) for m in members]
                + [guest_landed[m, h].astype(F32) for m in guests],
            ).astype(BF16)
    first_ref[...] = out.astype(BF16)
    exchanged(reads, landed, sp_size - 1, out_sem, 0)

    @pl.when(host)
    def _():
        exchanged(reads, guest_staged, sp_size - 1, guest_sem, 2)


def settle(cache_ref, first_ref, cache_out, first_out):
    cache_out[...] = cache_ref[...]
    first_out[...] = first_ref[...]


def on_device(
    layer_input, key_weight, value_weight, decay_exponent, query_new, key_new, value_new, norm_gain
):
    tokens, feats = layer_input.shape
    parts = lax.axis_size("tp")
    sp_size = lax.axis_size("sp")
    seq_span = sp_size // SEQS
    side = math.isqrt(parts)
    heads = decay_exponent.shape[0]
    width = key_weight.shape[1] // heads
    vwidth = value_weight.shape[1] // heads
    kept = width // sp_size
    room = tokens + 2 * SLIP
    groups = heads // next(p for p in (4, 2, 1) if heads % p == 0)
    steps = np.linspace(0.0, 1.0, width // 2, dtype=np.float32)
    inverse = (np.float32(1.0) / np.power(np.float32(10000.0), steps)).astype(np.float32)
    inverse = jnp.asarray(np.concatenate([inverse, inverse])[None, :])
    anywhere = pl.BlockSpec(memory_space=pltpu.HBM)
    vmem = pl.BlockSpec(memory_space=pltpu.VMEM)
    held = [
        pltpu.with_memory_space_constraint(part, pltpu.HBM)
        for part in (
            decay_exponent, inverse, query_new, key_new, value_new, norm_gain.reshape(1, -1),
            layer_input, key_weight, value_weight,
        )
    ]
    state_cache, first_read = pl.pallas_call(
        functools.partial(gather_kernel, side, seq_span, CHUNKS),
        out_shape=(
            jax.ShapeDtypeStruct((SEQS, heads, kept, vwidth), BF16),
            jax.ShapeDtypeStruct((SEQS, heads * vwidth), BF16),
        ),
        in_specs=[anywhere] * 9,
        out_specs=(vmem, vmem),
        scratch_shapes=[
            pltpu.SMEM((heads,), F32),
            pltpu.VMEM(inverse.shape, F32),
            pltpu.VMEM((3,) + query_new.shape, BF16),
            pltpu.VMEM((1, heads * vwidth), F32),
            pltpu.VMEM((parts, room, feats), BF16),
            pltpu.VMEM((2,) + key_weight.shape, BF16),
            pltpu.VMEM((room, width), F32),
            pltpu.VMEM((room, width), F32),
            pltpu.VMEM((room, heads * width), F32),
            pltpu.VMEM((room, heads * vwidth), F32),
            pltpu.VMEM((heads, width, vwidth), F32),
            pltpu.VMEM((heads, tokens // CHUNKS, width), F32),
            pltpu.VMEM((heads, 1, vwidth), F32),
            pltpu.VMEM((heads, width, vwidth), F32),
            pltpu.VMEM((SEQS, heads, 1, vwidth), F32),
            pltpu.VMEM((heads, 1, vwidth), F32),
            pltpu.VMEM((sp_size, heads, kept, vwidth), BF16),
            pltpu.VMEM((sp_size, heads, kept, vwidth), BF16),
            pltpu.VMEM((heads, 1, vwidth), F32),
            pltpu.VMEM((sp_size, heads, 1, vwidth), F32),
            pltpu.VMEM((groups, tokens // CHUNKS, heads // groups * width), F32),
            pltpu.VMEM((groups, tokens // CHUNKS, heads // groups * vwidth), BF16),
            pltpu.VMEM((heads, 2 * SLIP, width), F32),
            pltpu.VMEM((heads, width, vwidth), F32),
            pltpu.VMEM((sp_size, heads, kept, vwidth), BF16),
            pltpu.VMEM((2, heads, kept, vwidth), BF16),
            pltpu.VMEM((heads, 1, vwidth), F32),
            pltpu.VMEM((2, heads, 1, vwidth), F32),
            pltpu.SemaphoreType.DMA((4 * (side - 1),)),
            pltpu.SemaphoreType.DMA((3, CHUNKS)),
            pltpu.SemaphoreType.DMA((2,)),
            pltpu.SemaphoreType.DMA((2, 3)),
            pltpu.SemaphoreType.DMA((7,)),
            pltpu.SemaphoreType.DMA((4,)),
            pltpu.SemaphoreType.DMA((6,)),
            pltpu.SemaphoreType.REGULAR,
            pltpu.SemaphoreType.REGULAR,
            pltpu.SemaphoreType.REGULAR,
            pltpu.SemaphoreType.REGULAR,
            pltpu.SemaphoreType.REGULAR,
        ],
        compiler_params=pltpu.CompilerParams(
            collective_id=0, has_side_effects=True, vmem_limit_bytes=VMEM_KIB * 1024
        ),
    )(*held)
    return pl.pallas_call(
        settle,
        out_shape=(
            jax.ShapeDtypeStruct(state_cache.shape, BF16),
            jax.ShapeDtypeStruct(first_read.shape, BF16),
        ),
        in_specs=[vmem, vmem],
        out_specs=(vmem, vmem),
        compiler_params=pltpu.CompilerParams(vmem_limit_bytes=4 * 1024 * 1024),
    )(state_cache, first_read)


def solution(mesh):
    in_specs = (
        P("sp", "tp"),
        P(None, "tp"),
        P(None, "tp"),
        P("tp"),
        P(None, "tp"),
        P(None, "tp"),
        P(None, "tp"),
        P("tp"),
    )
    out_specs = (P(None, "tp", "sp", None), P(None, "tp"))
    return jax.shard_map(
        on_device, mesh=mesh, in_specs=in_specs, out_specs=out_specs, check_vma=False
    )
```

```python
import functools
import math

import jax
import jax.numpy as jnp
import numpy as np
from jax import lax
from jax.experimental import pallas as pl
from jax.experimental.pallas import tpu as pltpu
from jax.sharding import PartitionSpec as P

SEQS = 2
CHUNKS = (1, 1, 2, 2, 1, 1)
LEAD = 1
SLIP = 16
VMEM_KIB = 48 * 1024
MESH = pl.DeviceIdType.MESH
F32 = jnp.float32
BF16 = jnp.bfloat16


def gather_kernel(
    side, seq_span,
    decay_hbm, inv_hbm, query_hbm, key_hbm, value_hbm, gain_hbm, x_ref, wk_ref, wv_ref,
    cache_ref, first_ref,
    decay_ref, inv_ref, fresh_ref, gain_ref,
    gx, w_ref, cosine, sine, acc_k, acc_v,
    state_ref, fade, shrink, query_wide, own_term, factor, staged, landed, read, reads,
    k_tmp, v_tmp, guest_fade, guest_wide, guest_staged, guest_landed, guest_read, guest_reads,
    send_sem, recv_sem, slip_send, slip_recv, local_sem, out_sem, guest_sem,
    go_sem, ready_sem, x_sem, y_sem, mate_sem,
):
    tokens, feats = x_ref.shape
    unit = tokens // sum(CHUNKS)
    sizes = [unit * n for n in CHUNKS]
    slip = SLIP
    ahead = 2 * slip
    starts = [ahead + unit * sum(CHUNKS[:c]) for c in range(len(CHUNKS))]
    longest = max(sizes)
    last = len(CHUNKS) - 1
    heads, width, vwidth = state_ref.shape
    pair = next(p for p in (4, 2, 1) if heads % p == 0)
    me = lax.axis_index("tp")
    my_y, my_x = me // side, lax.rem(me, side)
    sp_place = lax.axis_index("sp")
    sp_size = landed.shape[0]
    kept = landed.shape[2]
    groups = heads // pair
    core = lax.rem(sp_place, 2)
    shift = sp_size - 2
    donor, host = sp_place >= shift, sp_place < 2
    full = jnp.logical_not(donor)

    sp_peers = [jnp.where(sp_place > p, p, p + 1) for p in range(sp_size - 1)]

    def x_peer(d):
        return my_y * side + lax.rem(my_x + d, side)

    def y_peer(d):
        return lax.rem(my_y + d, side) * side + my_x

    x_peers = [x_peer(d) for d in range(1, side)]
    y_peers = [y_peer(d) for d in range(1, side)]
    late_blocks = [
        lax.rem(my_y + dy, side) * side + lax.rem(my_x + dx, side)
        for dy in range(1, side)
        for dx in range(1, side)
    ]
    early_blocks = [me] + x_peers + y_peers

    def fetch(first):
        start, count = (0, sizes[0]) if first else (sizes[0], tokens - sizes[0])
        return pltpu.make_async_copy(
            x_ref.at[pl.ds(start, count)], gx.at[me, pl.ds(ahead + start, count)],
            local_sem.at[0 if first else 1],
        )

    fetch(True).start()
    barrier = pltpu.get_barrier_semaphore()
    below = sp_place - core
    above = below + 2

    def tell(semaphore, axis, peer):
        pl.semaphore_signal(semaphore, inc=1, device_id={axis: peer}, device_id_type=MESH)

    def expect(semaphore, count):
        @pl.when(count > 0)
        def _():
            pl.semaphore_wait(semaphore, count)

    for peer in x_peers + y_peers:
        pl.when(peer > me)(functools.partial(tell, barrier, "tp", peer))

    @pl.when(core == 0)
    def _():
        tell(barrier, "sp", sp_place + 1)

    def greet(peer, _):
        tell(barrier, "sp", peer)
        return 0

    lax.fori_loop(above, sp_size, greet, 0)
    expect(barrier, my_x + my_y + sp_place)
    for peer in x_peers:
        pl.when(peer < me)(functools.partial(tell, x_sem, "tp", peer))
    for peer in y_peers:
        pl.when(peer < me)(functools.partial(tell, y_sem, "tp", peer))

    @pl.when(core == 1)
    def _():
        tell(mate_sem, "sp", sp_place - 1)

    fetch(True).wait()
    fetch(False).start()

    def answer(peer, _):
        tell(ready_sem, "sp", peer)
        return 0

    def chunk_plot(c):
        half = sizes[c] // 2
        return (
            lambda part: starts[c] + part * half,
            half - slip if c == last else half,
            lambda slot: send_sem.at[slot], lambda kind: recv_sem.at[kind, c],
        )

    def slip_plot(which):
        return (
            lambda part: part * slip if which else starts[last] + (part + 1) * (sizes[last] // 2) - slip,
            slip, lambda slot: slip_send.at[which], lambda kind: slip_recv.at[which, kind],
        )

    plots = [chunk_plot(c) for c in range(last + 1)]
    tail_plot, guest_plot = slip_plot(0), slip_plot(1)

    def remote(plot, slot, block, part, target, kind):
        start, count, send, recv = plot
        where = (block, pl.ds(start(part), count))
        return pltpu.make_async_remote_copy(
            src_ref=gx.at[where],
            dst_ref=gx.at[where],
            send_sem=send(slot),
            recv_sem=recv(kind),
            device_id={"tp": target},
            device_id_type=MESH,
        )

    fan = 2 * (side - 1)

    def along(plot, wave, on_x):
        part = wave if on_x else 1 - wave
        first = 0 if on_x else side - 1
        return [
            remote(plot, first + slot, me, part, peer, wave)
            for slot, peer in enumerate(x_peers if on_x else y_peers)
        ]

    def own_copies(plot, wave):
        return along(plot, wave, True) + along(plot, wave, False)

    def relay_copies(plot):
        out, slot = [], fan
        for part, sources, peers in ((0, x_peers, y_peers), (1, y_peers, x_peers)):
            for peer in peers:
                for source in sources:
                    out.append(remote(plot, slot, source, part, peer, 2))
                slot += 1
        return out

    def arrived(plot, kind):
        blocks = (side - 1) ** 2 if kind == 2 else side - 1
        spot = gx.at[pl.ds(0, blocks), pl.ds(0, 2 * plot[1])]
        pltpu.make_async_copy(spot, spot, plot[3](kind)).wait()

    def start_all(copies):
        for copy in copies:
            copy.start()

    def settled(blocks, count, semaphore):
        spot = gx.at[pl.ds(0, blocks), pl.ds(0, count)]
        pltpu.make_async_copy(spot, spot, semaphore).wait()

    def lend():
        return [
            pltpu.make_async_remote_copy(
                src_ref=gx.at[me, pl.ds(tail_plot[0](part), slip)],
                dst_ref=gx.at[me, pl.ds(guest_plot[0](part), slip)],
                send_sem=guest_sem.at[0],
                recv_sem=guest_sem.at[1],
                device_id={"sp": sp_place - shift},
                device_id_type=MESH,
            )
            for part in range(2)
        ]

    @pl.when(core == 1)
    def _():
        pl.semaphore_wait(go_sem, 1)

    def send_first(on_x):
        start_all(along(plots[0], 0, on_x))

    x_last, y_last = my_x == side - 1, my_y == side - 1
    pl.when(x_last)(functools.partial(send_first, True))
    pl.when(y_last)(functools.partial(send_first, False))

    @pl.when(jnp.logical_not(x_last))
    def _():
        expect(x_sem, side - 1 - my_x)
        send_first(True)

    @pl.when(jnp.logical_not(y_last))
    def _():
        expect(y_sem, side - 1 - my_y)
        send_first(False)

    fetch(False).wait()

    @pl.when(donor)
    def _():
        start_all(lend())
        for block in x_peers + y_peers + late_blocks:
            for part in range(2):
                gx[block, pl.ds(tail_plot[0](part), slip), :] = jnp.zeros((slip, feats), BF16)

    def send_own(wave):
        for plot in plots[1 - wave:]:
            start_all(own_copies(plot, wave))

        @pl.when(full)
        def _():
            start_all(own_copies(tail_plot, wave))

    send_own(0)
    lax.fori_loop(0, below, answer, 0)

    small = [
        pltpu.make_async_copy(source, target, local_sem.at[2 + i])
        for i, (source, target) in enumerate((
            (decay_hbm, decay_ref), (inv_hbm, inv_ref), (gain_hbm, gain_ref),
        ))
    ]
    fresh = [
        pltpu.make_async_copy(source, fresh_ref.at[i], local_sem.at[5])
        for i, source in enumerate((query_hbm, key_hbm, value_hbm))
    ]
    weights = [
        pltpu.make_async_copy(source, w_ref.at[i], local_sem.at[6])
        for i, source in enumerate((wk_ref, wv_ref))
    ]
    start_all(small)
    start_all(fresh)
    start_all(weights)
    state_ref[...] = jnp.zeros_like(state_ref)

    def pass_on(plot):
        arrived(plot, 0)
        start_all(relay_copies(plot))

    for plot in plots[:LEAD]:
        pass_on(plot)

    @pl.when(core == 0)
    def _():
        pl.semaphore_wait(mate_sem, 1)
        tell(go_sem, "sp", sp_place + 1)

    for copy in small:
        copy.wait()
    pltpu.make_async_copy(fresh_ref, fresh_ref, local_sem.at[5]).wait()
    base = lax.rem(sp_place, seq_span) * tokens
    guest_place = lax.rem(sp_place + shift, sp_size)
    guest_base = lax.rem(guest_place, seq_span) * tokens
    scale = width ** (-0.5)

    def fill(at, count, first):
        place = (first + lax.broadcasted_iota(jnp.int32, (count, width), 0)).astype(F32)
        angle = place * inv_ref[...]
        low = lax.broadcasted_iota(jnp.int32, (count, width), 1) < width // 2
        sin = jnp.sin(angle) * scale
        cosine[pl.ds(at, count), :] = jnp.cos(angle) * scale
        sine[pl.ds(at, count), :] = jnp.where(low, -sin, sin)

    def table(c, _):
        at = pl.multiple_of(ahead + c * (unit // 2), math.gcd(ahead, unit // 2))
        fill(at, unit // 2, base + c * (unit // 2))
        return 0

    lax.fori_loop(0, 2 * sum(CHUNKS), table, 0)

    def to_end(first, count):
        return ((seq_span * tokens - 1 - first) - lax.broadcasted_iota(
            jnp.int32, (count, width), 0
        )).astype(F32)

    distance = to_end(base + tokens - longest, longest)
    spans = sorted(set(CHUNKS))

    def fading(h, _):
        fade[h] = jnp.exp(decay_ref[h] * distance)
        for k, n in enumerate(spans):
            shrink[k, h] = jnp.exp(jnp.full((1, vwidth), decay_ref[h] * (unit * n), F32))
        return 0

    lax.fori_loop(0, heads, fading, 0)

    diagonal = lax.broadcasted_iota(jnp.int32, (width, width), 0) == lax.broadcasted_iota(
        jnp.int32, (width, width), 1
    )
    ones = jnp.ones((width, vwidth), BF16)
    queries, next_keys, next_values = (fresh_ref[i].astype(F32) for i in range(3))

    def widen(target, prompt):
        for h in range(heads):
            mine = jnp.zeros((1, width), F32)
            for s in range(SEQS):
                mine = jnp.where(
                    prompt == s, queries[s:s + 1, h * width:(h + 1) * width], mine
                )
            spread = jnp.where(
                diagonal, jnp.broadcast_to(mine, (width, width)), 0.0
            ).astype(BF16)
            target[h] = jnp.dot(spread, ones, preferred_element_type=F32)

    widen(query_wide, sp_place // seq_span)
    for h in range(heads):
        cols = slice(h * width, (h + 1) * width)
        for s in range(SEQS):
            score = jnp.sum(
                queries[s:s + 1, cols] * next_keys[s:s + 1, cols], axis=1, keepdims=True
            )
            own_term[s, h] = score * next_values[s:s + 1, h * vwidth:(h + 1) * vwidth]
        factor[h] = jnp.exp(jnp.full((1, vwidth), decay_ref[h], F32))

    @pl.when(donor)
    def _():
        for part in range(2):
            at = pl.ds(tail_plot[0](part), slip)
            cosine[at, :] = jnp.zeros((slip, width), F32)
            sine[at, :] = jnp.zeros((slip, width), F32)

    @pl.when(host)
    def _():
        settled(1, 2 * slip, guest_sem.at[1])
        for wave in range(2):
            start_all(own_copies(guest_plot, wave))

    send_own(1)

    @pl.when(host)
    def _():
        for part in range(2):
            first = guest_base + tail_plot[0](part) - ahead
            fill(guest_plot[0](part), slip, first)
            gap = to_end(first, slip)
            for h in range(heads):
                guest_fade[h, pl.ds(part * slip, slip), :] = jnp.exp(decay_ref[h] * gap)
        widen(guest_wide, guest_place // seq_span)

    def outgoing(g, state, state_to, gist, gist_to, semaphores, at, peers=None):
        piece = pl.ds(g * pair, pair)
        out = []
        for peer in peers or sp_peers:
            for k, (source, target) in enumerate((
                (gist.at[piece], gist_to.at[sp_place, piece]),
                (state.at[peer, piece], state_to.at[sp_place, piece]),
            )):
                out.append(pltpu.make_async_remote_copy(
                    src_ref=source,
                    dst_ref=target,
                    send_sem=semaphores.at[at + 2 * k],
                    recv_sem=semaphores.at[at + 2 * k + 1],
                    device_id={"sp": peer},
                    device_id_type=MESH,
                ))
        return out

    pltpu.make_async_copy(w_ref, w_ref, local_sem.at[6]).wait()
    wk, wv = w_ref.at[0], w_ref.at[1]

    def partial(at, blocks, w, cols):
        total = None
        for block in blocks:
            depth = pl.ds(pl.multiple_of(block * feats, feats), feats)
            term = jnp.dot(gx[block, at, :], w[depth, cols], preferred_element_type=F32)
            total = term if total is None else total + term
        return total

    def columns(g):
        return (
            pl.ds(pl.multiple_of(g * pair * width, pair * width), pair * width),
            pl.ds(pl.multiple_of(g * pair * vwidth, pair * vwidth), pair * vwidth),
        )

    def chunk_rows(c):
        return pl.ds(starts[c], sizes[c])

    first_rows = pl.ds(0, starts[0] + sizes[0])

    def begin(at):
        def step(g, _):
            kcols, vcols = columns(g)
            acc_k[at, kcols] = partial(at, early_blocks, wk, kcols)
            acc_v[at, vcols] = partial(at, early_blocks, wv, vcols)
            return 0

        lax.fori_loop(0, groups, step, 0)

    def multiply(g, at):
        some = pl.ds(0, at.size)
        kcols = pl.ds(g * pair * width, pair * width)
        vcols = pl.ds(g * pair * vwidth, pair * vwidth)
        k_tmp[g, some, :] = partial(at, late_blocks, wk, kcols) + acc_k[at, kcols]
        v_tmp[g, some, :] = (
            partial(at, late_blocks, wv, vcols) + acc_v[at, vcols]
        ).astype(BF16)

    def absorb(g, at, some, weigh, keep):
        past = weigh.shape[1] - at.size
        for j in range(pair):
            kh = k_tmp[g, some, j * width:(j + 1) * width]
            turned = kh * cosine[at, :] + pltpu.roll(kh, width // 2, 1) * sine[at, :]
            keep(g * pair + j, lax.dot_general(
                (turned * weigh[g * pair + j, past:, :]).astype(BF16),
                v_tmp[g, some, j * vwidth:(j + 1) * vwidth],
                (((0,), (0,)), ((), ())), preferred_element_type=F32,
            ))

    def finish(c, keep, after):
        at = chunk_rows(c)
        every, some = (at, pl.ds(0, sizes[c])) if c else (first_rows, at)
        multiply(0, every)
        for g in range(1, groups + 1):
            if g < groups:
                multiply(g, every)
            absorb(g - 1, at, some, fade, keep)
            after(g - 1)

    def carry_on(c, h, update):
        return state_ref[h] * shrink[spans.index(CHUNKS[c]), h] + update

    def late(c):
        def keep(h, update):
            state_ref[h] = carry_on(c, h, update)

        arrived(plots[c], 2)
        finish(c, keep, lambda g: None)

    def cut_up(h, held, wide, state, gist):
        for d in range(sp_size):
            state[d, h] = held[d * kept:(d + 1) * kept, :].astype(BF16)
        gist[h] = jnp.sum(wide[h] * held, axis=0, keepdims=True)

    middle = LEAD
    for plot in plots[LEAD:middle]:
        pass_on(plot)

    pl.when(host)(functools.partial(pass_on, guest_plot))
    for plot in plots[middle:]:
        pass_on(plot)
    pl.when(full)(functools.partial(pass_on, tail_plot))
    pl.when(host)(functools.partial(arrived, guest_plot, 1))
    for c, plot in enumerate(plots):
        arrived(plot, 1)
        if c == last:
            pl.when(full)(functools.partial(arrived, tail_plot, 1))
        begin(chunk_rows(c) if c else first_rows)
    expect(ready_sem, sp_size - above)

    pl.when(host)(functools.partial(arrived, guest_plot, 2))
    late(0)

    @pl.when(host)
    def _():
        guest_rows = pl.ds(0, ahead)
        for g in range(groups):
            absorb(
                g, guest_rows, guest_rows, guest_fade,
                lambda h, held: cut_up(h, held, guest_wide, guest_staged, guest_read),
            )
            start_all(outgoing(
                g, guest_staged, guest_landed, guest_read, guest_reads, guest_sem, 2
            ))
        guest_landed[sp_place] = guest_staged[sp_place]
        guest_reads[sp_place] = guest_read[...]

    for c in range(1, last):
        late(c)

    def deal(g):
        to = (staged, landed, read, reads, out_sem, 0)
        start_all(outgoing(g, *to, sp_peers[:2]))
        if g == groups - 1:
            for k in range(groups):
                start_all(outgoing(k, *to, sp_peers[2:]))

    for slot in range(fan):
        settled(1, tokens - 2 * slip, send_sem.at[slot])
    arrived(plots[last], 2)
    pl.when(full)(functools.partial(arrived, tail_plot, 2))
    finish(
        last,
        lambda h, update: cut_up(h, carry_on(last, h, update), query_wide, staged, read),
        deal,
    )

    landed[sp_place] = staged[sp_place]
    reads[sp_place] = read[...]
    for slot in range(fan):
        settled(side - 1, tokens // 2 - slip, send_sem.at[fan + slot])
    moved = (4 * (side - 1) + 2 * (side - 1) ** 2) * slip
    pl.when(full)(functools.partial(settled, 1, moved, slip_send.at[0]))
    pl.when(donor)(functools.partial(settled, 1, 2 * slip, guest_sem.at[0]))
    pl.when(host)(functools.partial(settled, 1, moved, slip_send.at[1]))

    def exchanged(gist, state, count, semaphores, at):
        some = pl.ds(0, count)
        for k, target in enumerate((gist, state)):
            pltpu.make_async_copy(
                target.at[some], target.at[some], semaphores.at[at + 2 * k]
            ).wait()

    pl.when(host)(functools.partial(exchanged, guest_reads, guest_landed, 1, guest_sem, 3))
    pl.when(jnp.logical_not(host))(
        functools.partial(exchanged, guest_reads, guest_landed, 2, guest_sem, 3)
    )
    exchanged(reads, landed, sp_size - 1, out_sem, 1)
    row = lax.broadcasted_iota(jnp.int32, (SEQS, heads * vwidth), 0)
    out = jnp.zeros((SEQS, heads * vwidth), F32)
    for s in range(SEQS):
        members = range(s * seq_span, (s + 1) * seq_span)
        guests = range(2) if s == SEQS - 1 else ()
        carried = functools.reduce(
            jnp.add, [reads[m] for m in members] + [guest_reads[m] for m in guests]
        )
        mixed = factor[...] * carried + own_term[s]
        normed = mixed * lax.rsqrt(jnp.mean(mixed * mixed, axis=2, keepdims=True) + 1e-06)
        line = jnp.concatenate([normed[h] for h in range(heads)], axis=1) * gain_ref[...]
        out = jnp.where(row == s, jnp.broadcast_to(line, out.shape), out)
        for h in range(heads):
            cache_ref[s, h] = functools.reduce(
                jnp.add,
                [landed[m, h].astype(F32) for m in members]
                + [guest_landed[m, h].astype(F32) for m in guests],
            ).astype(BF16)
    first_ref[...] = out.astype(BF16)
    exchanged(reads, landed, sp_size - 1, out_sem, 0)

    @pl.when(host)
    def _():
        exchanged(reads, guest_staged, sp_size - 1, guest_sem, 2)


def settle(cache_ref, first_ref, cache_out, first_out):
    cache_out[...] = cache_ref[...]
    first_out[...] = first_ref[...]


def on_device(
    layer_input, key_weight, value_weight, decay_exponent, query_new, key_new, value_new, norm_gain
):
    tokens, feats = layer_input.shape
    parts = lax.axis_size("tp")
    sp_size = lax.axis_size("sp")
    seq_span = sp_size // SEQS
    side = math.isqrt(parts)
    heads = decay_exponent.shape[0]
    width = key_weight.shape[1] // heads
    vwidth = value_weight.shape[1] // heads
    kept = width // sp_size
    room = tokens + 2 * SLIP
    longest = tokens // sum(CHUNKS) * max(CHUNKS)
    groups = heads // next(p for p in (4, 2, 1) if heads % p == 0)
    steps = np.linspace(0.0, 1.0, width // 2, dtype=np.float32)
    inverse = (np.float32(1.0) / np.power(np.float32(10000.0), steps)).astype(np.float32)
    inverse = jnp.asarray(np.concatenate([inverse, inverse])[None, :])
    anywhere = pl.BlockSpec(memory_space=pltpu.HBM)
    vmem = pl.BlockSpec(memory_space=pltpu.VMEM)
    held = [
        pltpu.with_memory_space_constraint(part, pltpu.HBM)
        for part in (
            decay_exponent, inverse, query_new, key_new, value_new, norm_gain.reshape(1, -1),
            layer_input, key_weight, value_weight,
        )
    ]
    state_cache, first_read = pl.pallas_call(
        functools.partial(gather_kernel, side, seq_span),
        out_shape=(
            jax.ShapeDtypeStruct((SEQS, heads, kept, vwidth), BF16),
            jax.ShapeDtypeStruct((SEQS, heads * vwidth), BF16),
        ),
        in_specs=[anywhere] * 9,
        out_specs=(vmem, vmem),
        scratch_shapes=[
            pltpu.SMEM((heads,), F32),
            pltpu.VMEM(inverse.shape, F32),
            pltpu.VMEM((3,) + query_new.shape, BF16),
            pltpu.VMEM((1, heads * vwidth), F32),
            pltpu.VMEM((parts, room, feats), BF16),
            pltpu.VMEM((2,) + key_weight.shape, BF16),
            pltpu.VMEM((room, width), F32),
            pltpu.VMEM((room, width), F32),
            pltpu.VMEM((room, heads * width), F32),
            pltpu.VMEM((room, heads * vwidth), F32),
            pltpu.VMEM((heads, width, vwidth), F32),
            pltpu.VMEM((heads, longest, width), F32),
            pltpu.VMEM((len(set(CHUNKS)), heads, 1, vwidth), F32),
            pltpu.VMEM((heads, width, vwidth), F32),
            pltpu.VMEM((SEQS, heads, 1, vwidth), F32),
            pltpu.VMEM((heads, 1, vwidth), F32),
            pltpu.VMEM((sp_size, heads, kept, vwidth), BF16),
            pltpu.VMEM((sp_size, heads, kept, vwidth), BF16),
            pltpu.VMEM((heads, 1, vwidth), F32),
            pltpu.VMEM((sp_size, heads, 1, vwidth), F32),
            pltpu.VMEM((groups, longest, heads // groups * width), F32),
            pltpu.VMEM((groups, longest, heads // groups * vwidth), BF16),
            pltpu.VMEM((heads, 2 * SLIP, width), F32),
            pltpu.VMEM((heads, width, vwidth), F32),
            pltpu.VMEM((sp_size, heads, kept, vwidth), BF16),
            pltpu.VMEM((2, heads, kept, vwidth), BF16),
            pltpu.VMEM((heads, 1, vwidth), F32),
            pltpu.VMEM((2, heads, 1, vwidth), F32),
            pltpu.SemaphoreType.DMA((4 * (side - 1),)),
            pltpu.SemaphoreType.DMA((3, len(CHUNKS))),
            pltpu.SemaphoreType.DMA((2,)),
            pltpu.SemaphoreType.DMA((2, 3)),
            pltpu.SemaphoreType.DMA((7,)),
            pltpu.SemaphoreType.DMA((4,)),
            pltpu.SemaphoreType.DMA((6,)),
            pltpu.SemaphoreType.REGULAR,
            pltpu.SemaphoreType.REGULAR,
            pltpu.SemaphoreType.REGULAR,
            pltpu.SemaphoreType.REGULAR,
            pltpu.SemaphoreType.REGULAR,
        ],
        compiler_params=pltpu.CompilerParams(
            collective_id=0, has_side_effects=True, vmem_limit_bytes=VMEM_KIB * 1024
        ),
    )(*held)
    return pl.pallas_call(
        settle,
        out_shape=(
            jax.ShapeDtypeStruct(state_cache.shape, BF16),
            jax.ShapeDtypeStruct(first_read.shape, BF16),
        ),
        in_specs=[vmem, vmem],
        out_specs=(vmem, vmem),
        compiler_params=pltpu.CompilerParams(vmem_limit_bytes=4 * 1024 * 1024),
    )(state_cache, first_read)


def solution(mesh):
    in_specs = (
        P("sp", "tp"),
        P(None, "tp"),
        P(None, "tp"),
        P("tp"),
        P(None, "tp"),
        P(None, "tp"),
        P(None, "tp"),
        P("tp"),
    )
    out_specs = (P(None, "tp", "sp", None), P(None, "tp"))
    return jax.shard_map(
        on_device, mesh=mesh, in_specs=in_specs, out_specs=out_specs, check_vma=False
    )
```

```python
import functools
import math

import jax
import jax.numpy as jnp
import numpy as np
from jax import lax
from jax.experimental import pallas as pl
from jax.experimental.pallas import tpu as pltpu
from jax.sharding import PartitionSpec as P

SEQS = 2
CHUNKS = (1, 1, 2, 2, 1, 1)
LEAD = 1
SLIP = 16
VMEM_KIB = 48 * 1024
MESH = pl.DeviceIdType.MESH
F32 = jnp.float32
BF16 = jnp.bfloat16


def gather_kernel(
    side, seq_span,
    decay_hbm, inv_hbm, query_hbm, key_hbm, value_hbm, gain_hbm, x_ref, wk_ref, wv_ref,
    cache_ref, first_ref,
    decay_ref, inv_ref, fresh_ref, gain_ref,
    gx, w_ref, cosine, sine, acc_k, acc_v,
    state_ref, fade, shrink, query_wide, own_term, factor, staged, landed, read, reads,
    k_tmp, v_tmp, guest_fade, guest_wide, guest_staged, guest_landed, guest_read, guest_reads,
    send_sem, recv_sem, slip_send, slip_recv, local_sem, out_sem, guest_sem,
    go_sem, ready_sem, x_sem, y_sem, mate_sem,
):
    tokens, feats = x_ref.shape
    unit = tokens // sum(CHUNKS)
    sizes = [unit * n for n in CHUNKS]
    slip = SLIP
    ahead = 2 * slip
    starts = [ahead + unit * sum(CHUNKS[:c]) for c in range(len(CHUNKS))]
    longest = max(sizes)
    last = len(CHUNKS) - 1
    heads, width, vwidth = state_ref.shape
    pair = next(p for p in (4, 2, 1) if heads % p == 0)
    me = lax.axis_index("tp")
    my_y, my_x = me // side, lax.rem(me, side)
    sp_place = lax.axis_index("sp")
    sp_size = landed.shape[0]
    kept = landed.shape[2]
    groups = heads // pair
    core = lax.rem(sp_place, 2)
    shift = sp_size - 2
    donor, host = sp_place >= shift, sp_place < 2
    full = jnp.logical_not(donor)

    sp_peers = [jnp.where(sp_place > p, p, p + 1) for p in range(sp_size - 1)]

    def x_peer(d):
        return my_y * side + lax.rem(my_x + d, side)

    def y_peer(d):
        return lax.rem(my_y + d, side) * side + my_x

    x_peers = [x_peer(d) for d in range(1, side)]
    y_peers = [y_peer(d) for d in range(1, side)]
    late_blocks = [
        lax.rem(my_y + dy, side) * side + lax.rem(my_x + dx, side)
        for dy in range(1, side)
        for dx in range(1, side)
    ]
    early_blocks = [me] + x_peers + y_peers

    def fetch(first):
        start, count = (0, sizes[0]) if first else (sizes[0], tokens - sizes[0])
        return pltpu.make_async_copy(
            x_ref.at[pl.ds(start, count)], gx.at[me, pl.ds(ahead + start, count)],
            local_sem.at[0 if first else 1],
        )

    fetch(True).start()
    barrier = pltpu.get_barrier_semaphore()
    below = sp_place - core
    above = below + 2

    def tell(semaphore, axis, peer):
        pl.semaphore_signal(semaphore, inc=1, device_id={axis: peer}, device_id_type=MESH)

    def expect(semaphore, count):
        @pl.when(count > 0)
        def _():
            pl.semaphore_wait(semaphore, count)

    for peer in x_peers + y_peers:
        pl.when(peer > me)(functools.partial(tell, barrier, "tp", peer))

    @pl.when(core == 0)
    def _():
        tell(barrier, "sp", sp_place + 1)

    def greet(peer, _):
        tell(barrier, "sp", peer)
        return 0

    lax.fori_loop(above, sp_size, greet, 0)
    expect(barrier, my_x + my_y + sp_place)
    for peer in x_peers:
        pl.when(peer < me)(functools.partial(tell, x_sem, "tp", peer))
    for peer in y_peers:
        pl.when(peer < me)(functools.partial(tell, y_sem, "tp", peer))

    @pl.when(core == 1)
    def _():
        tell(mate_sem, "sp", sp_place - 1)

    fetch(True).wait()
    fetch(False).start()

    def answer(peer, _):
        tell(ready_sem, "sp", peer)
        return 0

    def chunk_plot(c):
        half = sizes[c] // 2
        return (
            lambda part: starts[c] + part * half,
            half - slip if c == last else half,
            lambda slot: send_sem.at[slot], lambda kind: recv_sem.at[kind, c],
        )

    def slip_plot(which):
        return (
            lambda part: part * slip if which else starts[last] + (part + 1) * (sizes[last] // 2) - slip,
            slip, lambda slot: slip_send.at[which], lambda kind: slip_recv.at[which, kind],
        )

    plots = [chunk_plot(c) for c in range(last + 1)]
    tail_plot, guest_plot = slip_plot(0), slip_plot(1)

    def remote(plot, slot, block, part, target, kind):
        start, count, send, recv = plot
        where = (block, pl.ds(start(part), count))
        return pltpu.make_async_remote_copy(
            src_ref=gx.at[where],
            dst_ref=gx.at[where],
            send_sem=send(slot),
            recv_sem=recv(kind),
            device_id={"tp": target},
            device_id_type=MESH,
        )

    fan = 2 * (side - 1)

    def along(plot, wave, on_x):
        part = wave if on_x else 1 - wave
        first = 0 if on_x else side - 1
        return [
            remote(plot, first + slot, me, part, peer, wave)
            for slot, peer in enumerate(x_peers if on_x else y_peers)
        ]

    def own_copies(plot, wave):
        return along(plot, wave, True) + along(plot, wave, False)

    def relay_copies(plot):
        out, slot = [], fan
        for part, sources, peers in ((0, x_peers, y_peers), (1, y_peers, x_peers)):
            for peer in peers:
                for source in sources:
                    out.append(remote(plot, slot, source, part, peer, 2))
                slot += 1
        return out

    def arrived(plot, kind):
        blocks = (side - 1) ** 2 if kind == 2 else side - 1
        spot = gx.at[pl.ds(0, blocks), pl.ds(0, 2 * plot[1])]
        pltpu.make_async_copy(spot, spot, plot[3](kind)).wait()

    def start_all(copies):
        for copy in copies:
            copy.start()

    def settled(blocks, count, semaphore):
        spot = gx.at[pl.ds(0, blocks), pl.ds(0, count)]
        pltpu.make_async_copy(spot, spot, semaphore).wait()

    def lend():
        return [
            pltpu.make_async_remote_copy(
                src_ref=gx.at[me, pl.ds(tail_plot[0](part), slip)],
                dst_ref=gx.at[me, pl.ds(guest_plot[0](part), slip)],
                send_sem=guest_sem.at[0],
                recv_sem=guest_sem.at[1],
                device_id={"sp": sp_place - shift},
                device_id_type=MESH,
            )
            for part in range(2)
        ]

    @pl.when(core == 1)
    def _():
        pl.semaphore_wait(go_sem, 1)

    def send_first(on_x):
        start_all(along(plots[0], 0, on_x))

    x_last, y_last = my_x == side - 1, my_y == side - 1
    pl.when(x_last)(functools.partial(send_first, True))
    pl.when(y_last)(functools.partial(send_first, False))

    @pl.when(jnp.logical_not(x_last))
    def _():
        expect(x_sem, side - 1 - my_x)
        send_first(True)

    @pl.when(jnp.logical_not(y_last))
    def _():
        expect(y_sem, side - 1 - my_y)
        send_first(False)

    fetch(False).wait()

    @pl.when(donor)
    def _():
        start_all(lend())
        for block in x_peers + y_peers + late_blocks:
            for part in range(2):
                gx[block, pl.ds(tail_plot[0](part), slip), :] = jnp.zeros((slip, feats), BF16)

    def send_own(wave):
        for plot in plots[1 - wave:]:
            start_all(own_copies(plot, wave))

        @pl.when(full)
        def _():
            start_all(own_copies(tail_plot, wave))

    send_own(0)
    lax.fori_loop(0, below, answer, 0)

    small = [
        pltpu.make_async_copy(source, target, local_sem.at[2 + i])
        for i, (source, target) in enumerate((
            (decay_hbm, decay_ref), (inv_hbm, inv_ref), (gain_hbm, gain_ref),
        ))
    ]
    fresh = [
        pltpu.make_async_copy(source, fresh_ref.at[i], local_sem.at[5])
        for i, source in enumerate((query_hbm, key_hbm, value_hbm))
    ]
    weights = [
        pltpu.make_async_copy(source, w_ref.at[i], local_sem.at[6])
        for i, source in enumerate((wk_ref, wv_ref))
    ]
    start_all(small)
    start_all(fresh)
    start_all(weights)
    state_ref[...] = jnp.zeros_like(state_ref)

    def pass_on(plot):
        arrived(plot, 0)
        start_all(relay_copies(plot))

    for plot in plots[:LEAD]:
        pass_on(plot)

    @pl.when(core == 0)
    def _():
        pl.semaphore_wait(mate_sem, 1)
        tell(go_sem, "sp", sp_place + 1)

    for copy in small:
        copy.wait()
    pltpu.make_async_copy(fresh_ref, fresh_ref, local_sem.at[5]).wait()
    base = lax.rem(sp_place, seq_span) * tokens
    guest_place = lax.rem(sp_place + shift, sp_size)
    guest_base = lax.rem(guest_place, seq_span) * tokens
    scale = width ** (-0.5)

    def fill(at, count, first):
        place = (first + lax.broadcasted_iota(jnp.int32, (count, width), 0)).astype(F32)
        angle = place * inv_ref[...]
        low = lax.broadcasted_iota(jnp.int32, (count, width), 1) < width // 2
        sin = jnp.sin(angle) * scale
        cosine[pl.ds(at, count), :] = jnp.cos(angle) * scale
        sine[pl.ds(at, count), :] = jnp.where(low, -sin, sin)

    def table(c, _):
        at = pl.multiple_of(ahead + c * (unit // 2), math.gcd(ahead, unit // 2))
        fill(at, unit // 2, base + c * (unit // 2))
        return 0

    lax.fori_loop(0, 2 * sum(CHUNKS), table, 0)

    def to_end(first, count):
        return ((seq_span * tokens - 1 - first) - lax.broadcasted_iota(
            jnp.int32, (count, width), 0
        )).astype(F32)

    distance = to_end(base + tokens - longest, longest)
    spans = sorted(set(CHUNKS))

    def fading(h, _):
        fade[h] = jnp.exp(decay_ref[h] * distance)
        for k, n in enumerate(spans):
            shrink[k, h] = jnp.exp(jnp.full((1, vwidth), decay_ref[h] * (unit * n), F32))
        return 0

    lax.fori_loop(0, heads, fading, 0)

    diagonal = lax.broadcasted_iota(jnp.int32, (width, width), 0) == lax.broadcasted_iota(
        jnp.int32, (width, width), 1
    )
    ones = jnp.ones((width, vwidth), BF16)
    queries, next_keys, next_values = (fresh_ref[i].astype(F32) for i in range(3))

    def widen(target, prompt):
        for h in range(heads):
            mine = jnp.zeros((1, width), F32)
            for s in range(SEQS):
                mine = jnp.where(
                    prompt == s, queries[s:s + 1, h * width:(h + 1) * width], mine
                )
            spread = jnp.where(
                diagonal, jnp.broadcast_to(mine, (width, width)), 0.0
            ).astype(BF16)
            target[h] = jnp.dot(spread, ones, preferred_element_type=F32)

    widen(query_wide, sp_place // seq_span)
    for h in range(heads):
        cols = slice(h * width, (h + 1) * width)
        for s in range(SEQS):
            score = jnp.sum(
                queries[s:s + 1, cols] * next_keys[s:s + 1, cols], axis=1, keepdims=True
            )
            own_term[s, h] = score * next_values[s:s + 1, h * vwidth:(h + 1) * vwidth]
        factor[h] = jnp.exp(jnp.full((1, vwidth), decay_ref[h], F32))

    @pl.when(donor)
    def _():
        for part in range(2):
            at = pl.ds(tail_plot[0](part), slip)
            cosine[at, :] = jnp.zeros((slip, width), F32)
            sine[at, :] = jnp.zeros((slip, width), F32)

    @pl.when(host)
    def _():
        settled(1, 2 * slip, guest_sem.at[1])
        for wave in range(2):
            start_all(own_copies(guest_plot, wave))

    send_own(1)

    @pl.when(host)
    def _():
        for part in range(2):
            first = guest_base + tail_plot[0](part) - ahead
            fill(guest_plot[0](part), slip, first)
            gap = to_end(first, slip)
            for h in range(heads):
                guest_fade[h, pl.ds(part * slip, slip), :] = jnp.exp(decay_ref[h] * gap)
        widen(guest_wide, guest_place // seq_span)

    def outgoing(g, state, state_to, gist, gist_to, semaphores, at, peers=None):
        piece = pl.ds(g * pair, pair)
        out = []
        for peer in peers or sp_peers:
            for k, (source, target) in enumerate((
                (gist, gist_to.at[sp_place]),
                (state.at[peer, piece], state_to.at[sp_place, piece]),
            )):
                if k == 0 and g < groups - 1:
                    continue
                out.append(pltpu.make_async_remote_copy(
                    src_ref=source,
                    dst_ref=target,
                    send_sem=semaphores.at[at + 2 * k],
                    recv_sem=semaphores.at[at + 2 * k + 1],
                    device_id={"sp": peer},
                    device_id_type=MESH,
                ))
        return out

    pltpu.make_async_copy(w_ref, w_ref, local_sem.at[6]).wait()
    wk, wv = w_ref.at[0], w_ref.at[1]

    def partial(at, blocks, w, cols):
        total = None
        for block in blocks:
            depth = pl.ds(pl.multiple_of(block * feats, feats), feats)
            term = jnp.dot(gx[block, at, :], w[depth, cols], preferred_element_type=F32)
            total = term if total is None else total + term
        return total

    def columns(g):
        return (
            pl.ds(pl.multiple_of(g * pair * width, pair * width), pair * width),
            pl.ds(pl.multiple_of(g * pair * vwidth, pair * vwidth), pair * vwidth),
        )

    def chunk_rows(c):
        return pl.ds(starts[c], sizes[c])

    first_rows = pl.ds(0, starts[0] + sizes[0])

    def begin(at):
        def step(g, _):
            kcols, vcols = columns(g)
            acc_k[at, kcols] = partial(at, early_blocks, wk, kcols)
            acc_v[at, vcols] = partial(at, early_blocks, wv, vcols)
            return 0

        lax.fori_loop(0, groups, step, 0)

    def multiply(g, at):
        some = pl.ds(0, at.size)
        kcols = pl.ds(g * pair * width, pair * width)
        vcols = pl.ds(g * pair * vwidth, pair * vwidth)
        k_tmp[g, some, :] = partial(at, late_blocks, wk, kcols) + acc_k[at, kcols]
        v_tmp[g, some, :] = (
            partial(at, late_blocks, wv, vcols) + acc_v[at, vcols]
        ).astype(BF16)

    def absorb(g, at, some, weigh, keep):
        past = weigh.shape[1] - at.size
        for j in range(pair):
            kh = k_tmp[g, some, j * width:(j + 1) * width]
            turned = kh * cosine[at, :] + pltpu.roll(kh, width // 2, 1) * sine[at, :]
            keep(g * pair + j, lax.dot_general(
                (turned * weigh[g * pair + j, past:, :]).astype(BF16),
                v_tmp[g, some, j * vwidth:(j + 1) * vwidth],
                (((0,), (0,)), ((), ())), preferred_element_type=F32,
            ))

    def finish(c, keep, after):
        at = chunk_rows(c)
        every, some = (at, pl.ds(0, sizes[c])) if c else (first_rows, at)
        multiply(0, every)
        for g in range(1, groups + 1):
            if g < groups and c < last:
                multiply(g, every)
            absorb(g - 1, at, some, fade, keep)
            after(g - 1)
            if g < groups and c == last:
                multiply(g, every)

    def carry_on(c, h, update):
        return state_ref[h] * shrink[spans.index(CHUNKS[c]), h] + update

    def late(c):
        def keep(h, update):
            state_ref[h] = carry_on(c, h, update)

        arrived(plots[c], 2)
        finish(c, keep, lambda g: None)

    def cut_up(h, held, wide, state, gist):
        for d in range(sp_size):
            state[d, h] = held[d * kept:(d + 1) * kept, :].astype(BF16)
        gist[h] = jnp.sum(wide[h] * held, axis=0, keepdims=True)

    middle = LEAD
    for plot in plots[LEAD:middle]:
        pass_on(plot)

    pl.when(host)(functools.partial(pass_on, guest_plot))
    for plot in plots[middle:]:
        pass_on(plot)
    pl.when(full)(functools.partial(pass_on, tail_plot))
    pl.when(host)(functools.partial(arrived, guest_plot, 1))
    for c, plot in enumerate(plots):
        arrived(plot, 1)
        if c == last:
            pl.when(full)(functools.partial(arrived, tail_plot, 1))
        begin(chunk_rows(c) if c else first_rows)
    expect(ready_sem, sp_size - above)

    pl.when(host)(functools.partial(arrived, guest_plot, 2))
    late(0)

    @pl.when(host)
    def _():
        guest_rows = pl.ds(0, ahead)
        for g in range(groups):
            absorb(
                g, guest_rows, guest_rows, guest_fade,
                lambda h, held: cut_up(h, held, guest_wide, guest_staged, guest_read),
            )
            start_all(outgoing(
                g, guest_staged, guest_landed, guest_read, guest_reads, guest_sem, 2
            ))
        guest_landed[sp_place] = guest_staged[sp_place]
        guest_reads[sp_place] = guest_read[...]

    for c in range(1, last):
        late(c)

    def deal(g):
        to = (staged, landed, read, reads, out_sem, 0)
        start_all(outgoing(g, *to, sp_peers[:4]))
        if g == groups - 1:
            for k in range(groups):
                start_all(outgoing(k, *to, sp_peers[4:]))

    for slot in range(fan):
        settled(1, tokens - 2 * slip, send_sem.at[slot])
    arrived(plots[last], 2)
    pl.when(full)(functools.partial(arrived, tail_plot, 2))
    finish(
        last,
        lambda h, update: cut_up(h, carry_on(last, h, update), query_wide, staged, read),
        deal,
    )

    landed[sp_place] = staged[sp_place]
    reads[sp_place] = read[...]
    for slot in range(fan):
        settled(side - 1, tokens // 2 - slip, send_sem.at[fan + slot])
    moved = (4 * (side - 1) + 2 * (side - 1) ** 2) * slip
    pl.when(full)(functools.partial(settled, 1, moved, slip_send.at[0]))
    pl.when(donor)(functools.partial(settled, 1, 2 * slip, guest_sem.at[0]))
    pl.when(host)(functools.partial(settled, 1, moved, slip_send.at[1]))

    def exchanged(gist, state, count, semaphores, at):
        some = pl.ds(0, count)
        for k, target in enumerate((gist, state)):
            pltpu.make_async_copy(
                target.at[some], target.at[some], semaphores.at[at + 2 * k]
            ).wait()

    pl.when(host)(functools.partial(exchanged, guest_reads, guest_landed, 1, guest_sem, 3))
    pl.when(jnp.logical_not(host))(
        functools.partial(exchanged, guest_reads, guest_landed, 2, guest_sem, 3)
    )
    exchanged(reads, landed, sp_size - 1, out_sem, 1)
    row = lax.broadcasted_iota(jnp.int32, (SEQS, heads * vwidth), 0)
    out = jnp.zeros((SEQS, heads * vwidth), F32)
    for s in range(SEQS):
        members = range(s * seq_span, (s + 1) * seq_span)
        guests = range(2) if s == SEQS - 1 else ()
        carried = functools.reduce(
            jnp.add, [reads[m] for m in members] + [guest_reads[m] for m in guests]
        )
        mixed = factor[...] * carried + own_term[s]
        normed = mixed * lax.rsqrt(jnp.mean(mixed * mixed, axis=2, keepdims=True) + 1e-06)
        line = jnp.concatenate([normed[h] for h in range(heads)], axis=1) * gain_ref[...]
        out = jnp.where(row == s, jnp.broadcast_to(line, out.shape), out)
        for h in range(heads):
            cache_ref[s, h] = functools.reduce(
                jnp.add,
                [landed[m, h].astype(F32) for m in members]
                + [guest_landed[m, h].astype(F32) for m in guests],
            ).astype(BF16)
    first_ref[...] = out.astype(BF16)
    exchanged(reads, landed, sp_size - 1, out_sem, 0)

    @pl.when(host)
    def _():
        exchanged(reads, guest_staged, sp_size - 1, guest_sem, 2)


def settle(cache_ref, first_ref, cache_out, first_out):
    cache_out[...] = cache_ref[...]
    first_out[...] = first_ref[...]


def on_device(
    layer_input, key_weight, value_weight, decay_exponent, query_new, key_new, value_new, norm_gain
):
    tokens, feats = layer_input.shape
    parts = lax.axis_size("tp")
    sp_size = lax.axis_size("sp")
    seq_span = sp_size // SEQS
    side = math.isqrt(parts)
    heads = decay_exponent.shape[0]
    width = key_weight.shape[1] // heads
    vwidth = value_weight.shape[1] // heads
    kept = width // sp_size
    room = tokens + 2 * SLIP
    longest = tokens // sum(CHUNKS) * max(CHUNKS)
    groups = heads // next(p for p in (4, 2, 1) if heads % p == 0)
    steps = np.linspace(0.0, 1.0, width // 2, dtype=np.float32)
    inverse = (np.float32(1.0) / np.power(np.float32(10000.0), steps)).astype(np.float32)
    inverse = jnp.asarray(np.concatenate([inverse, inverse])[None, :])
    anywhere = pl.BlockSpec(memory_space=pltpu.HBM)
    vmem = pl.BlockSpec(memory_space=pltpu.VMEM)
    held = [
        pltpu.with_memory_space_constraint(part, pltpu.HBM)
        for part in (
            decay_exponent, inverse, query_new, key_new, value_new, norm_gain.reshape(1, -1),
            layer_input, key_weight, value_weight,
        )
    ]
    state_cache, first_read = pl.pallas_call(
        functools.partial(gather_kernel, side, seq_span),
        out_shape=(
            jax.ShapeDtypeStruct((SEQS, heads, kept, vwidth), BF16),
            jax.ShapeDtypeStruct((SEQS, heads * vwidth), BF16),
        ),
        in_specs=[anywhere] * 9,
        out_specs=(vmem, vmem),
        scratch_shapes=[
            pltpu.SMEM((heads,), F32),
            pltpu.VMEM(inverse.shape, F32),
            pltpu.VMEM((3,) + query_new.shape, BF16),
            pltpu.VMEM((1, heads * vwidth), F32),
            pltpu.VMEM((parts, room, feats), BF16),
            pltpu.VMEM((2,) + key_weight.shape, BF16),
            pltpu.VMEM((room, width), F32),
            pltpu.VMEM((room, width), F32),
            pltpu.VMEM((room, heads * width), F32),
            pltpu.VMEM((room, heads * vwidth), F32),
            pltpu.VMEM((heads, width, vwidth), F32),
            pltpu.VMEM((heads, longest, width), F32),
            pltpu.VMEM((len(set(CHUNKS)), heads, 1, vwidth), F32),
            pltpu.VMEM((heads, width, vwidth), F32),
            pltpu.VMEM((SEQS, heads, 1, vwidth), F32),
            pltpu.VMEM((heads, 1, vwidth), F32),
            pltpu.VMEM((sp_size, heads, kept, vwidth), BF16),
            pltpu.VMEM((sp_size, heads, kept, vwidth), BF16),
            pltpu.VMEM((heads, 1, vwidth), F32),
            pltpu.VMEM((sp_size, heads, 1, vwidth), F32),
            pltpu.VMEM((groups, longest, heads // groups * width), F32),
            pltpu.VMEM((groups, longest, heads // groups * vwidth), BF16),
            pltpu.VMEM((heads, 2 * SLIP, width), F32),
            pltpu.VMEM((heads, width, vwidth), F32),
            pltpu.VMEM((sp_size, heads, kept, vwidth), BF16),
            pltpu.VMEM((2, heads, kept, vwidth), BF16),
            pltpu.VMEM((heads, 1, vwidth), F32),
            pltpu.VMEM((2, heads, 1, vwidth), F32),
            pltpu.SemaphoreType.DMA((4 * (side - 1),)),
            pltpu.SemaphoreType.DMA((3, len(CHUNKS))),
            pltpu.SemaphoreType.DMA((2,)),
            pltpu.SemaphoreType.DMA((2, 3)),
            pltpu.SemaphoreType.DMA((7,)),
            pltpu.SemaphoreType.DMA((4,)),
            pltpu.SemaphoreType.DMA((6,)),
            pltpu.SemaphoreType.REGULAR,
            pltpu.SemaphoreType.REGULAR,
            pltpu.SemaphoreType.REGULAR,
            pltpu.SemaphoreType.REGULAR,
            pltpu.SemaphoreType.REGULAR,
        ],
        compiler_params=pltpu.CompilerParams(
            collective_id=0, has_side_effects=True, vmem_limit_bytes=VMEM_KIB * 1024
        ),
    )(*held)
    return pl.pallas_call(
        settle,
        out_shape=(
            jax.ShapeDtypeStruct(state_cache.shape, BF16),
            jax.ShapeDtypeStruct(first_read.shape, BF16),
        ),
        in_specs=[vmem, vmem],
        out_specs=(vmem, vmem),
        compiler_params=pltpu.CompilerParams(vmem_limit_bytes=4 * 1024 * 1024),
    )(state_cache, first_read)


def solution(mesh):
    in_specs = (
        P("sp", "tp"),
        P(None, "tp"),
        P(None, "tp"),
        P("tp"),
        P(None, "tp"),
        P(None, "tp"),
        P(None, "tp"),
        P("tp"),
    )
    out_specs = (P(None, "tp", "sp", None), P(None, "tp"))
    return jax.shard_map(
        on_device, mesh=mesh, in_specs=in_specs, out_specs=out_specs, check_vma=False
    )
```
